512 devices in a mesh: ep: 32 (over z, x), tp: 16 (over y, core).
Axes of the slice: x: 4, y: 8, z: 8, core: 2. Of those that a mesh axis runs over, the one named last changes fastest.
Arguments:
- mix_input: bfloat16 [16384, 2048], P('ep', 'tp'), may hold values from -6 to 6
- mix_weight: bfloat16 [2048, 4096], P(None, 'tp'), may hold values from -0.125 to 0.125
- expert_input: bfloat16 [4096, 4096], P('ep', 'tp'), may hold values from -4500 to 4500
- expert_index: int32 [4096, 2], P('ep'), may hold values from 0 to 31, as said below
- route_share: float32 [4096, 2], P('ep'), may hold values from 0.1 to 1
- norm_gain: float32 [4096], replicated, may hold values from 0.1 to 1.9
- gate_weight: bfloat16 [32, 4096, 2048], P('ep', None, 'tp'), may hold values from -0.09375 to 0.09375
- up_weight: bfloat16 [32, 4096, 2048], P('ep', None, 'tp'), may hold values from -0.09375 to 0.09375
- down_weight: bfloat16 [32, 2048, 4096], P('ep', None, 'tp'), may hold values from -0.125 to 0.125
Outputs:
- mixed_rows: bfloat16 [16384, 4096], P('ep', 'tp')
- expert_rows: bfloat16 [4096, 4096], P('ep', 'tp')
The draws below stay inside these ranges and needn't reach their ends.
Inputs may be any that keep to these rules, and one draw needn't show every extreme that they name: `expert_index`: each row names 2 different experts. Within each aligned block of 128 rows (the rows of one index of ep) no expert is named by more than 16 rows, and one expert, the same in every block, is named by exactly 16 rows.
All inputs are finite; a program needn't handle non-finite values.
Results may differ from the reference program's by a relative error of at most 0.007.
Values may be sent and summed in bfloat16 or wider, within the bound.
No kernel may reach another device: no remote copies, remote signals or barrier semaphores. Data moves between devices by JAX's collectives and lax.ppermute only.
A program may use at most 64 MiB of HBM per device.

```python
import math
from functools import partial
import jax
import jax.numpy as jnp
from jax import lax

D = 4096
POOL = 2048
FF = 2048
TOP = 2
TOK_EXP = 128
EXPERTS = 32
CAP = 16
TOKENS_MIX = 16384
TOKENS_EXP = 4096
N_EP = 32


def draw_expert_input(key, part):
    key_cols, key_rows, key_noise = jax.random.split(key, 3)
    column = jnp.arange(D, dtype=jnp.float32) / (D - 1)
    col_scale = jnp.exp(math.log(3.0) * column + jax.random.uniform(key_cols, (D,), jnp.float32, 0.0, math.log(10.0)))
    noise = jnp.clip(jax.random.normal(key_noise, (TOKENS_EXP, D), jnp.float32), -5.0, 5.0)
    row_scale = jnp.exp(jax.random.uniform(key_rows, (TOKENS_EXP, 1), jnp.float32, 0.0, math.log(10.0)))
    return (noise * col_scale[None, :] * row_scale).astype(jnp.bfloat16)


def draw_expert_index(key, part):
    key_full, key_rest = jax.random.split(key)
    favored = jax.random.randint(key_full, (), 0, EXPERTS)

    def one_block(block_key):
        key_order, key_rows, key_flip = jax.random.split(block_key, 3)
        others = jax.random.permutation(key_order, EXPERTS - 1).astype(jnp.int32)
        others = others + (others >= favored).astype(jnp.int32)
        row_number = jnp.arange(TOK_EXP, dtype=jnp.int32)
        first = jnp.where(row_number < CAP, favored, others[2 * row_number % (EXPERTS - 1)])
        second = jnp.where(row_number < CAP, others[row_number % (EXPERTS - 1)], others[(2 * row_number + 1) % (EXPERTS - 1)])
        flipped = jax.random.randint(key_flip, (TOK_EXP,), 0, 2)
        pairs = jnp.stack([jnp.where(flipped == 1, second, first), jnp.where(flipped == 1, first, second)], axis=1)
        shuffle = jax.random.permutation(key_rows, TOK_EXP)
        return pairs[shuffle]
    blocks = jax.vmap(one_block)(jax.random.split(key_rest, N_EP))
    return blocks.reshape(N_EP * TOK_EXP, 2).astype(jnp.int32)


def levels(own_key, shape, cuts, least, high):
    gain = 1.0
    for dim, shards_of in cuts:
        draws = jax.random.uniform(jax.random.fold_in(jax.random.fold_in(own_key, 6), dim), (shards_of,), jnp.float32, least / len(cuts), high / len(cuts))
        gain = gain * jnp.repeat(jnp.exp(draws), shape[dim] // shards_of).reshape((-1,) + (1,) * (len(shape) - 1 - dim))
    return gain


def normal_values(rng, shape, width, most, pieces=(), held_as=jnp.bfloat16):
    drawn = width * jax.random.normal(rng, shape, jnp.float32)
    if pieces:
        drawn = drawn * levels(rng, shape, pieces, -0.22, 0.18)
    return jnp.clip(drawn, -most, most).astype(held_as)


def setup_inputs(seed: int = 0) -> dict:
    key_of = jax.random.split(jax.random.key(seed), 10)
    mix_input = normal_values(key_of[0], (TOKENS_MIX, POOL), 1.0, 6.0, ((0, 32), (1, 16)))
    mix_weight = normal_values(key_of[1], (POOL, D), POOL ** -0.5, 0.125, ((1, 16),))
    expert_input = draw_expert_input(jax.random.fold_in(key_of[9], 71), 0)
    expert_index = draw_expert_index(jax.random.fold_in(key_of[9], 71), 0)
    route_share = jnp.clip(jnp.exp(math.log(1.0) - 2.3025851 * jax.random.uniform(key_of[4], (TOKENS_EXP, TOP), jnp.float32) ** levels(key_of[4], (TOKENS_EXP, TOP), ((0, 32),), -0.2, 0.2)), 0.1, 1.0)
    norm_gain = jnp.clip(1.0 + 0.18 * jax.random.normal(key_of[5], (D,), jnp.float32), 0.1, 1.9)
    gate_weight = normal_values(key_of[6], (EXPERTS, D, FF), D ** -0.5, 0.09375, ((0, 32), (2, 16)))
    up_weight = normal_values(key_of[7], (EXPERTS, D, FF), D ** -0.5, 0.09375, ((0, 32), (2, 16)))
    down_weight = normal_values(key_of[8], (EXPERTS, FF, D), FF ** -0.5, 0.125, ((0, 32), (2, 16)))
    return {"mix_input": mix_input, "mix_weight": mix_weight, "expert_input": expert_input, "expert_index": expert_index, "route_share": route_share, "norm_gain": norm_gain, "gate_weight": gate_weight, "up_weight": up_weight, "down_weight": down_weight}


window_reach = 15
norm_eps = 1e-06

def pool_minus_self(extended, first_pos, group_size, channel_base):
    length = extended.shape[0] - window_reach
    channels = extended.shape[1]
    channel = channel_base + jnp.arange(channels, dtype=jnp.int32)
    window = jnp.power(2, channel // group_size + 1).astype(jnp.int32)
    running = jnp.zeros((length, channels), jnp.float32)
    for lag_count in range(window_reach + 1):
        shifted = extended[window_reach - lag_count:window_reach - lag_count + length]
        running = running + jnp.where(lag_count < window[None, :], shifted, 0.0)
    position = first_pos + jnp.arange(length, dtype=jnp.int32)
    counts = jnp.minimum(position[:, None] + 1, window[None, :]).astype(jnp.float32)
    return (running / counts - extended[window_reach:]).astype(jnp.bfloat16)

def slot_targets(indices, experts, capacity):
    flattened = indices.reshape(-1)
    one_hot = (flattened[:, None] == jnp.arange(experts, dtype=jnp.int32)[None, :]).astype(jnp.int32)
    earlier = jnp.cumsum(one_hot, axis=0) - one_hot
    return flattened * capacity + lax.optimization_barrier(jnp.sum(earlier * one_hot, axis=1))

def reference(mix_input, mix_weight, expert_input, expert_index, route_share, norm_gain, gate_weight, up_weight, down_weight):
    extended = jnp.pad(mix_input.astype(jnp.float32), ((window_reach, 0), (0, 0)))
    pooled = pool_minus_self(extended, 0, POOL // 4, 0)
    mixed_rows = jnp.dot(pooled, mix_weight, preferred_element_type=jnp.float32).astype(jnp.bfloat16)
    blocks = expert_index.reshape(N_EP, TOK_EXP, TOP)
    targets = jax.vmap(partial(slot_targets, experts=EXPERTS, capacity=CAP))(blocks)
    expert_of = targets // CAP
    slot_of = targets % CAP
    source = jnp.arange(N_EP, dtype=jnp.int32)[:, None]
    placed = (expert_of * (N_EP * CAP) + source * CAP + slot_of).reshape(-1)
    row_ids = (source * TOK_EXP + jnp.repeat(jnp.arange(TOK_EXP, dtype=jnp.int32), TOP)[None, :]).reshape(-1)
    table = jnp.full((EXPERTS * N_EP * CAP,), TOKENS_EXP, jnp.int32).at[placed].set(row_ids)
    padded = jnp.concatenate([expert_input, jnp.zeros((1, D), jnp.bfloat16)], axis=0)

    def run_expert(operands):
        identity, gate_mat, up_mat, down_mat = operands
        rows_in = padded[identity]
        squares = lax.optimization_barrier(jnp.mean(jnp.square(rows_in.astype(jnp.float32)), axis=1, keepdims=True))
        inverse = lax.rsqrt(squares + norm_eps)
        scaled = (rows_in.astype(jnp.float32) * norm_gain).astype(jnp.bfloat16)
        gate_acts = jnp.dot(scaled, gate_mat, preferred_element_type=jnp.float32) * inverse
        up_acts = jnp.dot(scaled, up_mat, preferred_element_type=jnp.float32) * inverse
        hidden = (jax.nn.silu(gate_acts) * up_acts).astype(jnp.bfloat16)
        return jnp.dot(hidden, down_mat, preferred_element_type=jnp.float32).astype(jnp.bfloat16)
    produced = lax.map(run_expert, (table.reshape(EXPERTS, N_EP * CAP), gate_weight, up_weight, down_weight))
    picked = produced.reshape(EXPERTS * N_EP * CAP, D)[placed].astype(jnp.float32).reshape(TOKENS_EXP, TOP, D)
    shares = route_share / lax.optimization_barrier(jnp.sum(route_share, axis=1, keepdims=True))
    expert_rows = lax.optimization_barrier(jnp.sum(picked * shares[:, :, None], axis=1)).astype(jnp.bfloat16)
    return (mixed_rows, expert_rows)
```

```python
import functools

import jax
import jax.numpy as jnp
from jax import lax
from jax.experimental import pallas as pl
from jax.experimental.pallas import tpu as pltpu
from jax.sharding import PartitionSpec as P

POOL = 2048
GROUPS = 4
TOP = 2
HALO = 16
norm_eps = 1e-06

VMEM = pl.BlockSpec(memory_space=pltpu.VMEM)
SMEM = pl.BlockSpec(memory_space=pltpu.SMEM)


def dot(a, b, dims=((1,), (0,))):
    return lax.dot_general(a, b, (dims, ((), ())), preferred_element_type=jnp.float32)


def slots_of(index, experts, capacity):
    tokens = index.shape[0]
    lanes = lax.broadcasted_iota(jnp.int32, (tokens, experts), 1)
    first, second = lanes == index[:, 0:1], lanes == index[:, 1:2]
    named = jnp.where(first | second, 1.0, 0.0)
    row = lax.broadcasted_iota(jnp.int32, (tokens, tokens), 0)
    col = lax.broadcasted_iota(jnp.int32, (tokens, tokens), 1)
    before = jnp.where(col < row, 1.0, 0.0).astype(jnp.bfloat16)
    earlier = dot(before, named.astype(jnp.bfloat16))
    slot = jnp.where(first | second, earlier, -1.0).astype(jnp.bfloat16)
    expert = lax.broadcasted_iota(jnp.int32, (experts, experts * capacity), 0)
    place = lax.broadcasted_iota(jnp.int32, (experts, experts * capacity), 1)
    spread = jnp.where(place // capacity == expert, 1.0, 0.0).astype(jnp.bfloat16)
    wanted = lax.broadcasted_iota(jnp.int32, (tokens, experts * capacity), 1) % capacity
    hit = dot(slot, spread) == wanted.astype(jnp.float32)
    return hit, first, second, spread


def dispatch_kernel(experts, capacity, index_ref, rows_ref, out_ref):
    hit, _, _, _ = slots_of(index_ref[...], experts, capacity)
    placed = jnp.where(hit, 1.0, 0.0).astype(jnp.bfloat16)
    out_ref[...] = dot(placed, rows_ref[...], ((0,), (0,))).astype(out_ref.dtype)


def dispatch(index, rows, experts, capacity):
    return pl.pallas_call(
        functools.partial(dispatch_kernel, experts, capacity),
        out_shape=jax.ShapeDtypeStruct((experts * capacity, rows.shape[1]), rows.dtype),
        in_specs=[VMEM, VMEM],
        out_specs=VMEM,
        name="dispatch",
        cost_estimate=pl.CostEstimate(flops=50_000_000, bytes_accessed=400_000, transcendentals=0),
    )(index, rows)


def shares_kernel(experts, capacity, index_ref, share_ref, high_ref, low_ref):
    hit, first, second, spread = slots_of(index_ref[...], experts, capacity)
    share = share_ref[...]
    share = share / (share[:, 0:1] + share[:, 1:2])
    by_expert = jnp.where(first, share[:, 0:1], jnp.where(second, share[:, 1:2], 0.0))
    high = by_expert.astype(jnp.bfloat16)
    low = (by_expert - high.astype(jnp.float32)).astype(jnp.bfloat16)
    high_ref[...] = jnp.where(hit, dot(high, spread), 0.0).astype(jnp.bfloat16)
    low_ref[...] = jnp.where(hit, dot(low, spread), 0.0).astype(jnp.bfloat16)


def weights_of_slots(index, share, experts, capacity):
    shape = jax.ShapeDtypeStruct((index.shape[0], experts * capacity), jnp.bfloat16)
    return pl.pallas_call(
        functools.partial(shares_kernel, experts, capacity),
        out_shape=(shape, shape),
        in_specs=[VMEM, VMEM],
        out_specs=(VMEM, VMEM),
        name="shares",
        cost_estimate=pl.CostEstimate(flops=20_000_000, bytes_accessed=300_000, transcendentals=0),
    )(index, share)


def combine_kernel(high_ref, low_ref, rows_ref, out_ref):
    rows = rows_ref[...]
    out_ref[...] = (dot(high_ref[...], rows) + dot(low_ref[...], rows)).astype(out_ref.dtype)


def combine(high, low, rows):
    return pl.pallas_call(
        combine_kernel,
        out_shape=jax.ShapeDtypeStruct((high.shape[0], rows.shape[1]), jnp.bfloat16),
        in_specs=[VMEM] * 3,
        out_specs=VMEM,
        name="combine",
        cost_estimate=pl.CostEstimate(flops=70_000_000, bytes_accessed=600_000, transcendentals=0),
    )(high, low, rows)


def pool_kernel(place_ref, before_ref, rows_ref, out_ref):
    rows = rows_ref[...].astype(jnp.float32)
    tokens = rows.shape[0]
    total = jnp.concatenate([before_ref[...].astype(jnp.float32), rows], axis=0)
    group = place_ref[1]
    window = 1
    picked = jnp.zeros_like(rows)
    for step in range(GROUPS):
        total = total + jnp.concatenate(
            [jnp.zeros((window, total.shape[1]), jnp.float32), total[:-window]], axis=0
        )
        window *= 2
        picked = jnp.where(group == step, total[HALO:], picked)
    position = place_ref[0] + lax.broadcasted_iota(jnp.int32, rows.shape, 0)
    width = jnp.left_shift(2, group)
    counts = jnp.minimum(position + 1, width).astype(jnp.float32)
    out_ref[...] = (picked / counts - rows).astype(out_ref.dtype)


def pool(place, before, rows):
    return pl.pallas_call(
        pool_kernel,
        out_shape=jax.ShapeDtypeStruct(rows.shape, rows.dtype),
        in_specs=[SMEM, VMEM, VMEM],
        out_specs=VMEM,
        name="pool",
        cost_estimate=pl.CostEstimate(flops=1_000_000, bytes_accessed=300_000, transcendentals=0),
    )(place, before, rows)


def hidden_kernel(blocks, width, rows_ref, gain_ref, gate_ref, up_ref, out_ref, gates, ups, squares):
    block = pl.program_id(0)
    rows = rows_ref[0].astype(jnp.float32)
    scaled = (rows * gain_ref[...]).astype(jnp.bfloat16)
    gate, up = dot(scaled, gate_ref[0]), dot(scaled, up_ref[0])
    square = jnp.square(rows)
    square = sum(square[:, at : at + 128] for at in range(0, rows.shape[1], 128))

    @pl.when(block == 0)
    def _():
        gates[...], ups[...], squares[...] = gate, up, square

    @pl.when(block > 0)
    def _():
        gates[...] += gate
        ups[...] += up
        squares[...] += square

    @pl.when(block == blocks - 1)
    def _():
        mean = jnp.sum(squares[...], axis=1, keepdims=True) / width
        inverse = lax.rsqrt(mean + norm_eps)
        gate_acts = gates[...] * inverse
        out_ref[...] = (gate_acts / (1.0 + jnp.exp(-gate_acts)) * (ups[...] * inverse)).astype(
            out_ref.dtype
        )


def hidden_of(gathered, gain, gate_weight, up_weight, features):
    blocks, rows, _ = gathered.shape
    hidden = gate_weight.shape[2]
    return pl.pallas_call(
        functools.partial(hidden_kernel, blocks, gain.shape[1]),
        out_shape=jax.ShapeDtypeStruct((rows, hidden), jnp.bfloat16),
        grid=(blocks,),
        in_specs=[
            pl.BlockSpec((1, rows, features), lambda k: (k, 0, 0)),
            pl.BlockSpec((1, features), lambda k: (0, k)),
            pl.BlockSpec((1, features, hidden), lambda k: (0, k, 0)),
            pl.BlockSpec((1, features, hidden), lambda k: (0, k, 0)),
        ],
        out_specs=pl.BlockSpec((rows, hidden), lambda k: (0, 0)),
        scratch_shapes=[
            pltpu.VMEM((rows, hidden), jnp.float32),
            pltpu.VMEM((rows, hidden), jnp.float32),
            pltpu.VMEM((rows, 128), jnp.float32),
        ],
        name="hidden",
        cost_estimate=pl.CostEstimate(
            flops=4 * rows * blocks * features * hidden, bytes_accessed=6_500_000, transcendentals=65536
        ),
    )(gathered, gain, gate_weight, up_weight)


def mix_kernel(blocks, rows_ref, weight_ref, out_ref, total):
    block = pl.program_id(0)
    part = dot(rows_ref[0], weight_ref[...])

    @pl.when(block == 0)
    def _():
        total[...] = part

    @pl.when(block > 0)
    def _():
        total[...] += part

    @pl.when(block == blocks - 1)
    def _():
        out_ref[...] = total[...].astype(out_ref.dtype)


def mixed_of(gathered, weight, first, channels):
    blocks, rows, _ = gathered.shape
    columns = weight.shape[1]
    return pl.pallas_call(
        functools.partial(mix_kernel, blocks),
        out_shape=jax.ShapeDtypeStruct((rows, columns), jnp.bfloat16),
        grid=(blocks,),
        in_specs=[
            pl.BlockSpec((1, rows, channels), lambda k: (k, 0, first // channels)),
            pl.BlockSpec((channels, columns), lambda k: (k, 0)),
        ],
        out_specs=pl.BlockSpec((rows, columns), lambda k: (0, 0)),
        scratch_shapes=[pltpu.VMEM((rows, columns), jnp.float32)],
        name="mixed",
        cost_estimate=pl.CostEstimate(
            flops=2 * rows * blocks * channels * columns, bytes_accessed=3_500_000, transcendentals=0
        ),
    )(gathered, weight)


def down_kernel(core_ref, own_ref, other_ref, own_weight_ref, other_weight_ref, out_ref, total):
    block = pl.program_id(0)
    part = dot(own_ref[0], own_weight_ref[0, 0]) + dot(other_ref[0], other_weight_ref[0, 0])

    @pl.when(block == 0)
    def _():
        total[...] = part

    @pl.when(block > 0)
    def _():
        total[...] += part

    @pl.when(block == pl.num_programs(0) - 1)
    def _():
        out_ref[...] = total[...].astype(out_ref.dtype)


def down(core, own, other, weight):
    blocks, rows, units = own.shape
    columns = weight.shape[3]
    return pl.pallas_call(
        down_kernel,
        grid_spec=pltpu.PrefetchScalarGridSpec(
            num_scalar_prefetch=1,
            grid=(blocks,),
            in_specs=[
                pl.BlockSpec((1, rows, units), lambda k, c: (k, 0, 0)),
                pl.BlockSpec((1, rows, units), lambda k, c: (k, 0, 0)),
                pl.BlockSpec((1, 1, units, columns), lambda k, c: (k, c[0], 0, 0)),
                pl.BlockSpec((1, 1, units, columns), lambda k, c: (k, 1 - c[0], 0, 0)),
            ],
            out_specs=pl.BlockSpec((rows, columns), lambda k, c: (0, 0)),
            scratch_shapes=[pltpu.VMEM((rows, columns), jnp.float32)],
        ),
        out_shape=jax.ShapeDtypeStruct((rows, columns), jnp.bfloat16),
        name="down",
        cost_estimate=pl.CostEstimate(
            flops=4 * rows * blocks * units * columns, bytes_accessed=3_500_000, transcendentals=0
        ),
    )(core, own, other, weight, weight)


def shards(
    mix_input,
    mix_weight,
    expert_input,
    expert_index,
    route_share,
    norm_gain,
    gate_weight,
    up_weight,
    down_weight,
):
    n_ep, n_tp = lax.axis_size("ep"), lax.axis_size("tp")
    chips = n_tp // 2
    ep, tp = lax.axis_index("ep"), lax.axis_index("tp")
    tokens_exp, features = expert_input.shape
    capacity = 2 * tokens_exp * TOP // n_ep

    outgoing = dispatch(expert_index, expert_input, n_ep, capacity)
    outgoing = outgoing.reshape(n_ep, capacity, features)
    arrived = lax.all_to_all(outgoing, "ep", 0, 0, tiled=True).reshape(n_ep * capacity, features)

    tokens_mix, channels = mix_input.shape
    before = lax.ppermute(
        mix_input[tokens_mix - HALO :], "ep", [(i, i + 1) for i in range(n_ep - 1)]
    )
    place = jnp.stack([ep * tokens_mix, tp * channels * GROUPS // POOL]).astype(jnp.int32)
    pooled = pool(place, before, mix_input)

    gathered = lax.all_gather(jnp.concatenate([arrived, pooled], axis=1), "tp", axis=0)
    hidden = hidden_of(gathered, norm_gain.reshape(1, -1), gate_weight, up_weight, features)
    mixed_rows = mixed_of(gathered, mix_weight, features, channels)

    columns_of_chips = [[chip * 2 + core for chip in range(chips)] for core in range(2)]
    partners = [(i, i + 1 - 2 * (i % 2)) for i in range(n_tp)]
    own = lax.all_to_all(
        jnp.broadcast_to(hidden[None], (chips, *hidden.shape)),
        "tp",
        0,
        0,
        tiled=True,
        axis_index_groups=columns_of_chips,
    )
    other = lax.ppermute(own, "tp", partners)
    core = (tp % 2).astype(jnp.int32).reshape(1)
    units = hidden.shape[1]
    produced = down(core, own, other, down_weight.reshape(chips, 2, units, down_weight.shape[2]))

    returned = lax.all_to_all(
        produced.reshape(n_ep, capacity, produced.shape[1]), "ep", 0, 0, tiled=True
    )
    high, low = weights_of_slots(expert_index, route_share, n_ep, capacity)
    expert_rows = combine(high, low, returned.reshape(n_ep * capacity, produced.shape[1]))
    return (mixed_rows, expert_rows)


def solution(mesh):
    placed = (
        P("ep", "tp"),
        P(None, "tp"),
        P("ep", "tp"),
        P("ep", None),
        P("ep", None),
        P(),
        P("ep", None, "tp"),
        P("ep", None, "tp"),
        P("ep", None, "tp"),
    )
    return jax.shard_map(
        shards,
        mesh=mesh,
        in_specs=placed,
        out_specs=(P("ep", "tp"), P("ep", "tp")),
        check_vma=False,
    )
```

```python
import functools

import jax
import jax.numpy as jnp
from jax import lax
from jax.experimental import pallas as pl
from jax.experimental.pallas import tpu as pltpu
from jax.sharding import PartitionSpec as P

POOL = 2048
GROUPS = 4
TOP = 2
HALO = 16
norm_eps = 1e-06

VMEM = pl.BlockSpec(memory_space=pltpu.VMEM)
SMEM = pl.BlockSpec(memory_space=pltpu.SMEM)
HBM = pl.BlockSpec(memory_space=pltpu.HBM)
EARLY = 112


def room(mib):
    return pltpu.CompilerParams(vmem_limit_bytes=mib * 2**20)


def cost(flops, moved):
    return pl.CostEstimate(flops=flops, bytes_accessed=moved, transcendentals=0)


def dot(a, b, dims=((1,), (0,))):
    return lax.dot_general(a, b, (dims, ((), ())), preferred_element_type=jnp.float32)


def slots_of(index, experts, capacity):
    tokens = index.shape[1]
    expert = lax.broadcasted_iota(jnp.int32, (experts, tokens), 0)
    first, second = expert == index[0:1], expert == index[1:2]
    named = jnp.where(first | second, 1.0, 0.0).astype(jnp.bfloat16)
    row = lax.broadcasted_iota(jnp.int32, (tokens, tokens), 0)
    col = lax.broadcasted_iota(jnp.int32, (tokens, tokens), 1)
    before = jnp.where(row < col, 1.0, 0.0).astype(jnp.bfloat16)
    slot = jnp.where(first | second, dot(named, before), -1.0).astype(jnp.bfloat16)
    place = lax.broadcasted_iota(jnp.int32, (experts * capacity, experts), 0)
    lane = lax.broadcasted_iota(jnp.int32, (experts * capacity, experts), 1)
    spread = jnp.where(place // capacity == lane, 1.0, 0.0).astype(jnp.bfloat16)
    wanted = lax.broadcasted_iota(jnp.int32, (experts * capacity, tokens), 0) % capacity
    hit = dot(spread, slot) == wanted.astype(jnp.float32)
    return hit, first, second, spread


def dispatch_kernel(experts, capacity, index_ref, rows_ref, out_ref):
    hit, _, _, _ = slots_of(index_ref[...], experts, capacity)
    placed = jnp.where(hit, 1.0, 0.0).astype(jnp.bfloat16)
    out_ref[...] = dot(placed, rows_ref[...]).astype(out_ref.dtype)


def dispatch(index, rows, experts, capacity):
    return pl.pallas_call(
        functools.partial(dispatch_kernel, experts, capacity),
        out_shape=jax.ShapeDtypeStruct((experts * capacity, rows.shape[1]), rows.dtype),
        in_specs=[VMEM, VMEM],
        out_specs=VMEM,
        name="dispatch",
        compiler_params=room(8),
        cost_estimate=cost(50_000_000, 400_000),
    )(index, rows)


def shares_kernel(experts, capacity, index_ref, share_ref, high_ref, low_ref):
    hit, first, second, spread = slots_of(index_ref[...], experts, capacity)
    share = share_ref[...]
    share = share / (share[0:1] + share[1:2])
    by_expert = jnp.where(first, share[0:1], jnp.where(second, share[1:2], 0.0))
    high = by_expert.astype(jnp.bfloat16)
    low = (by_expert - high.astype(jnp.float32)).astype(jnp.bfloat16)
    high_ref[...] = jnp.where(hit, dot(spread, high), 0.0).T.astype(jnp.bfloat16)
    low_ref[...] = jnp.where(hit, dot(spread, low), 0.0).T.astype(jnp.bfloat16)


def weights_of_slots(index, share, experts, capacity):
    shape = jax.ShapeDtypeStruct((index.shape[1], experts * capacity), jnp.bfloat16)
    return pl.pallas_call(
        functools.partial(shares_kernel, experts, capacity),
        out_shape=(shape, shape),
        in_specs=[VMEM, VMEM],
        out_specs=(VMEM, VMEM),
        name="shares",
        compiler_params=room(8),
        cost_estimate=cost(20_000_000, 300_000),
    )(index, share)


def combine_kernel(high_ref, low_ref, rows_ref, out_ref):
    rows = rows_ref[...]
    out_ref[...] = (dot(high_ref[...], rows) + dot(low_ref[...], rows)).astype(out_ref.dtype)


def combine(high, low, rows):
    return pl.pallas_call(
        combine_kernel,
        out_shape=jax.ShapeDtypeStruct((high.shape[0], rows.shape[1]), jnp.bfloat16),
        in_specs=[VMEM] * 3,
        out_specs=VMEM,
        name="combine",
        compiler_params=room(8),
        cost_estimate=cost(70_000_000, 600_000),
    )(high, low, rows)


def pool_kernel(place_ref, before_ref, rows_ref, out_ref):
    rows = rows_ref[...].astype(jnp.float32)
    total = jnp.concatenate([before_ref[...].astype(jnp.float32), rows], axis=0)
    group = place_ref[1]
    window = 1
    picked = jnp.zeros_like(rows)
    for step in range(GROUPS):
        total = total + jnp.concatenate(
            [jnp.zeros((window, total.shape[1]), jnp.float32), total[:-window]], axis=0
        )
        window *= 2
        picked = jnp.where(group == step, total[HALO:], picked)
    position = place_ref[0] + lax.broadcasted_iota(jnp.int32, rows.shape, 0)
    width = jnp.left_shift(2, group)
    counts = jnp.minimum(position + 1, width).astype(jnp.float32)
    out_ref[...] = (picked / counts - rows).astype(out_ref.dtype)


def pool(place, before, rows):
    return pl.pallas_call(
        pool_kernel,
        out_shape=jax.ShapeDtypeStruct(rows.shape, rows.dtype),
        in_specs=[SMEM, VMEM, VMEM],
        out_specs=VMEM,
        name="pool",
        compiler_params=room(8),
        cost_estimate=cost(1_000_000, 300_000),
    )(place, before, rows)


def side_by_side(blocks):
    return jnp.concatenate([blocks[i] for i in range(blocks.shape[0])], axis=1)


def finish(total, squares, width):
    units = total.shape[1] // 2
    inverse = lax.rsqrt(jnp.sum(squares, axis=1, keepdims=True) / width + norm_eps)
    gates, ups = total[:, :units] * inverse, total[:, units:] * inverse
    return (gates / (1.0 + jnp.exp(-gates)) * ups).astype(jnp.bfloat16)


def products(rows, gain, gate, up):
    rows = rows.astype(jnp.float32)
    scaled = (rows * gain).astype(jnp.bfloat16)
    square = jnp.square(rows)
    square = sum(square[:, at : at + 128] for at in range(0, rows.shape[1], 128))
    return dot(scaled, jnp.concatenate([gate, up], axis=1)), square


def early_kernel(rows_ref, gain_ref, gate_ref, up_ref, out_ref):
    total, square = products(side_by_side(rows_ref), gain_ref[...], gate_ref[0], up_ref[0])
    out_ref[...] = finish(total, square, gain_ref.shape[1])


def early_hidden_of(gathered, gain, gate_weight, up_weight):
    blocks, rows, features = gathered.shape
    units = gate_weight.shape[2]
    return pl.pallas_call(
        early_kernel,
        out_shape=jax.ShapeDtypeStruct((rows, units), jnp.bfloat16),
        in_specs=[VMEM] * 4,
        out_specs=VMEM,
        name="early_hidden",
        compiler_params=room(24),
        cost_estimate=cost(4 * rows * blocks * features * units, 3_500_000),
    )(gathered, gain, gate_weight, up_weight)


def fetch(source_ref, first, held, sems):
    copies = []
    for block in range(held.shape[0]):
        piece = source_ref.at[block, pl.ds(first, held.shape[1])]
        copies.append(pltpu.make_async_copy(piece, held.at[block], sems.at[block]))
        copies[-1].start()
    return copies


def hidden_kernel(
    at_once, from_ref, gain_ref, gate_from, up_from, out_ref, held, gate_ref, up_ref, sems, sides
):
    weights = [
        pltpu.make_async_copy(gate_from, gate_ref, sides.at[0]),
        pltpu.make_async_copy(up_from, up_ref, sides.at[1]),
    ]
    for weight in weights:
        weight.start()
    copies = fetch(from_ref, 0, held, sems)
    for weight in weights:
        weight.wait()
    rows = out_ref.shape[1]
    pieces = held.shape[1] // rows
    depth = at_once * pieces * held.shape[2]
    total = square = 0.0
    for step in range(len(copies) // at_once):
        parts = []
        for block in range(step * at_once, (step + 1) * at_once):
            copies[block].wait()
            parts += [held[block, i * rows : (i + 1) * rows] for i in range(pieces)]
        part = slice(step * depth, (step + 1) * depth)
        more, squares = products(
            jnp.concatenate(parts, axis=1), gain_ref[:, part], gate_ref[0, part], up_ref[0, part]
        )
        total, square = total + more, square + squares
    hidden = finish(total, square, gain_ref.shape[1])
    for copy in range(out_ref.shape[0]):
        out_ref[copy] = hidden


def hidden_of(gathered, gain, gate_weight, up_weight, rows, pieces, copies):
    blocks, _, lanes = gathered.shape
    units = gate_weight.shape[2]
    return pl.pallas_call(
        functools.partial(hidden_kernel, 4),
        out_shape=jax.ShapeDtypeStruct((copies, rows, units), jnp.bfloat16),
        in_specs=[HBM, VMEM, HBM, HBM],
        out_specs=VMEM,
        scratch_shapes=[
            pltpu.VMEM((blocks, pieces * rows, lanes), jnp.bfloat16),
            pltpu.VMEM(gate_weight.shape, jnp.bfloat16),
            pltpu.VMEM(up_weight.shape, jnp.bfloat16),
            pltpu.SemaphoreType.DMA((blocks,)),
            pltpu.SemaphoreType.DMA((2,)),
        ],
        name="hidden",
        compiler_params=room(60),
        cost_estimate=cost(4 * rows * gain.shape[1] * units, 6_500_000),
    )(gathered, gain, gate_weight, up_weight)


def mix_kernel(at_once, first, from_ref, weight_ref, out_ref, held, sems):
    copies = fetch(from_ref, first, held, sems)
    depth = at_once * held.shape[2]
    total = 0.0
    for step in range(len(copies) // at_once):
        parts = []
        for block in range(step * at_once, (step + 1) * at_once):
            copies[block].wait()
            parts.append(held[block])
        part = weight_ref[step * depth : (step + 1) * depth]
        total = total + dot(jnp.concatenate(parts, axis=1), part)
    out_ref[...] = total.astype(out_ref.dtype)


def mixed_of(gathered, weight, first, rows):
    blocks, _, lanes = gathered.shape
    columns = weight.shape[1]
    return pl.pallas_call(
        functools.partial(mix_kernel, 4, first),
        out_shape=jax.ShapeDtypeStruct((rows, columns), jnp.bfloat16),
        in_specs=[HBM, VMEM],
        out_specs=VMEM,
        scratch_shapes=[
            pltpu.VMEM((blocks, rows, lanes), jnp.bfloat16),
            pltpu.SemaphoreType.DMA((blocks,)),
        ],
        name="mixed",
        compiler_params=room(60),
        cost_estimate=cost(2 * rows * blocks * lanes * columns, 3_500_000),
    )(gathered, weight)


def down_kernel(core_ref, early_ref, own_ref, other_ref, weight_ref, out_ref):
    core = core_ref[0]
    chips = own_ref.shape[0]
    units = early_ref.shape[2]
    split = early_ref.shape[1]
    weight = weight_ref[...].reshape(2 * chips * units, weight_ref.shape[2])
    out_ref[:split] = dot(side_by_side(early_ref), weight).astype(out_ref.dtype)
    mine = jnp.concatenate([weight_ref[2 * i + core] for i in range(chips)], axis=0)
    total = dot(side_by_side(own_ref), mine)
    theirs = jnp.concatenate([weight_ref[2 * i + 1 - core] for i in range(chips)], axis=0)
    out_ref[split:] = (total + dot(side_by_side(other_ref), theirs)).astype(out_ref.dtype)


def down(core, early, own, other, weight):
    columns = weight.shape[2]
    rows = early.shape[1] + own.shape[1]
    return pl.pallas_call(
        down_kernel,
        in_specs=[SMEM, VMEM, VMEM, VMEM, VMEM],
        out_specs=VMEM,
        out_shape=jax.ShapeDtypeStruct((rows, columns), jnp.bfloat16),
        name="down",
        compiler_params=room(16),
        cost_estimate=cost(2 * rows * weight.shape[0] * weight.shape[1] * columns, 3_500_000),
    )(core, early, own, other, weight)


def shards(
    mix_input,
    mix_weight,
    expert_input,
    expert_index,
    route_share,
    norm_gain,
    gate_weight,
    up_weight,
    down_weight,
):
    n_ep, n_tp = lax.axis_size("ep"), lax.axis_size("tp")
    chips = n_tp // 2
    ep, tp = lax.axis_index("ep"), lax.axis_index("tp")
    tokens_exp, features = expert_input.shape
    capacity = 2 * tokens_exp * TOP // n_ep
    units = gate_weight.shape[2]
    index, share, gain = expert_index.T, route_share.T, norm_gain.reshape(1, -1)

    outgoing = dispatch(index, expert_input, n_ep, capacity)
    outgoing = outgoing.reshape(n_ep, capacity, features)
    arrived = lax.all_to_all(outgoing, "ep", 0, 0, tiled=True).reshape(n_ep * capacity, features)

    tokens_mix, channels = mix_input.shape
    before = lax.ppermute(
        mix_input[tokens_mix - HALO :], "ep", [(i, i + 1) for i in range(n_ep - 1)]
    )
    place = jnp.stack([ep * tokens_mix, tp // (POOL // GROUPS // channels)]).astype(jnp.int32)
    pooled = pool(place, before, mix_input)

    late_rows = n_ep * capacity - EARLY
    pieces = features // channels
    sent = [arrived[EARLY:, i * channels : (i + 1) * channels] for i in range(pieces)]
    gathered = lax.all_gather(jnp.concatenate(sent + [pooled], axis=0), "tp", axis=0)
    early = lax.all_gather(arrived[:EARLY], "tp", axis=0)
    early_hidden = early_hidden_of(early, gain, gate_weight, up_weight)
    early_hidden = lax.all_gather(early_hidden, "tp", axis=0)
    gathered, early_hidden = lax.optimization_barrier((gathered, early_hidden))
    hidden = hidden_of(gathered, gain, gate_weight, up_weight, late_rows, pieces, chips)
    mixed_rows = mixed_of(gathered, mix_weight, pieces * late_rows, tokens_mix)

    columns_of_chips = [[chip * 2 + core for chip in range(chips)] for core in range(2)]
    partners = [(i, i + 1 - 2 * (i % 2)) for i in range(n_tp)]
    own = lax.all_to_all(hidden, "tp", 0, 0, tiled=True, axis_index_groups=columns_of_chips)
    other = lax.ppermute(own, "tp", partners)
    core = lax.rem(tp, 2).astype(jnp.int32).reshape(1)
    produced = down(
        core, early_hidden, own, other, down_weight.reshape(n_tp, units, down_weight.shape[2])
    )

    returned = lax.all_to_all(
        produced.reshape(n_ep, capacity, produced.shape[1]), "ep", 0, 0, tiled=True
    )
    high, low = weights_of_slots(index, share, n_ep, capacity)
    expert_rows = combine(high, low, returned.reshape(n_ep * capacity, produced.shape[1]))
    return (mixed_rows, expert_rows)


def solution(mesh):
    placed = (
        P("ep", "tp"),
        P(None, "tp"),
        P("ep", "tp"),
        P("ep", None),
        P("ep", None),
        P(),
        P("ep", None, "tp"),
        P("ep", None, "tp"),
        P("ep", None, "tp"),
    )
    return jax.shard_map(
        shards,
        mesh=mesh,
        in_specs=placed,
        out_specs=(P("ep", "tp"), P("ep", "tp")),
        check_vma=False,
    )
```

```python
import functools

import jax
import jax.numpy as jnp
from jax import lax
from jax.experimental import pallas as pl
from jax.experimental.pallas import tpu as pltpu
from jax.sharding import PartitionSpec as P

POOL = 2048
GROUPS = 4
TOP = 2
HALO = 16
norm_eps = 1e-06

VMEM = pl.BlockSpec(memory_space=pltpu.VMEM)
SMEM = pl.BlockSpec(memory_space=pltpu.SMEM)
HBM = pl.BlockSpec(memory_space=pltpu.HBM)
HOLD = 588 * 2**20 // 10
EARLY = 112


def room(mib):
    return pltpu.CompilerParams(vmem_limit_bytes=mib * 2**20)


def cost(flops, moved):
    return pl.CostEstimate(flops=flops, bytes_accessed=moved, transcendentals=0)


def dot(a, b, dims=((1,), (0,))):
    return lax.dot_general(a, b, (dims, ((), ())), preferred_element_type=jnp.float32)


def slots_of(index, experts, capacity):
    tokens = index.shape[1]
    expert = lax.broadcasted_iota(jnp.int32, (experts, tokens), 0)
    first, second = expert == index[0:1], expert == index[1:2]
    named = jnp.where(first | second, 1.0, 0.0).astype(jnp.bfloat16)
    row = lax.broadcasted_iota(jnp.int32, (tokens, tokens), 0)
    col = lax.broadcasted_iota(jnp.int32, (tokens, tokens), 1)
    before = jnp.where(row < col, 1.0, 0.0).astype(jnp.bfloat16)
    slot = jnp.where(first | second, dot(named, before), -1.0).astype(jnp.bfloat16)
    place = lax.broadcasted_iota(jnp.int32, (experts * capacity, experts), 0)
    lane = lax.broadcasted_iota(jnp.int32, (experts * capacity, experts), 1)
    spread = jnp.where(place // capacity == lane, 1.0, 0.0).astype(jnp.bfloat16)
    wanted = lax.broadcasted_iota(jnp.int32, (experts * capacity, tokens), 0) % capacity
    hit = dot(spread, slot) == wanted.astype(jnp.float32)
    return hit, first, second, spread


def dispatch_kernel(experts, capacity, index_from, rows_from, out_ref, index_ref, rows_ref, sems):
    copies = [
        pltpu.make_async_copy(index_from, index_ref, sems.at[0]),
        pltpu.make_async_copy(rows_from, rows_ref, sems.at[1]),
    ]
    for copy in copies:
        copy.start()
    copies[0].wait()
    hit, _, _, _ = slots_of(index_ref[...], experts, capacity)
    placed = jnp.where(hit, 1.0, 0.0).astype(jnp.bfloat16)
    copies[1].wait()
    out_ref[...] = dot(placed, rows_ref[...]).astype(out_ref.dtype)


def dispatch(index, rows, experts, capacity):
    return pl.pallas_call(
        functools.partial(dispatch_kernel, experts, capacity),
        out_shape=jax.ShapeDtypeStruct((experts * capacity, rows.shape[1]), rows.dtype),
        in_specs=[HBM, HBM],
        out_specs=VMEM,
        scratch_shapes=[
            pltpu.VMEM(index.shape, index.dtype),
            pltpu.VMEM(rows.shape, rows.dtype),
            pltpu.SemaphoreType.DMA((2,)),
        ],
        name="dispatch",
        compiler_params=room(60),
        cost_estimate=cost(50_000_000, 400_000),
    )(index, rows)


def shares_kernel(experts, capacity, index_ref, share_ref, high_ref, low_ref):
    hit, first, second, spread = slots_of(index_ref[...], experts, capacity)
    share = share_ref[...]
    share = share / (share[0:1] + share[1:2])
    by_expert = jnp.where(first, share[0:1], jnp.where(second, share[1:2], 0.0))
    high = by_expert.astype(jnp.bfloat16)
    low = (by_expert - high.astype(jnp.float32)).astype(jnp.bfloat16)
    high_ref[...] = jnp.where(hit, dot(spread, high), 0.0).T.astype(jnp.bfloat16)
    low_ref[...] = jnp.where(hit, dot(spread, low), 0.0).T.astype(jnp.bfloat16)


def weights_of_slots(index, share, experts, capacity):
    shape = jax.ShapeDtypeStruct((index.shape[1], experts * capacity), jnp.bfloat16)
    return pl.pallas_call(
        functools.partial(shares_kernel, experts, capacity),
        out_shape=(shape, shape),
        in_specs=[VMEM, VMEM],
        out_specs=(VMEM, VMEM),
        name="shares",
        compiler_params=room(8),
        cost_estimate=cost(20_000_000, 300_000),
    )(index, share)


def combine_kernel(high_ref, low_ref, rows_ref, out_ref):
    rows = rows_ref[...]
    out_ref[...] = (dot(high_ref[...], rows) + dot(low_ref[...], rows)).astype(out_ref.dtype)


def combine(high, low, rows):
    return pl.pallas_call(
        combine_kernel,
        out_shape=jax.ShapeDtypeStruct((high.shape[0], rows.shape[1]), jnp.bfloat16),
        in_specs=[VMEM] * 3,
        out_specs=VMEM,
        name="combine",
        compiler_params=room(8),
        cost_estimate=cost(70_000_000, 600_000),
    )(high, low, rows)


def pool_kernel(place_ref, before_ref, rows_ref, out_ref):
    rows = rows_ref[...].astype(jnp.float32)
    total = jnp.concatenate([before_ref[...].astype(jnp.float32), rows], axis=0)
    group = place_ref[1]
    window = 1
    picked = jnp.zeros_like(rows)
    for step in range(GROUPS):
        total = total + jnp.concatenate(
            [jnp.zeros((window, total.shape[1]), jnp.float32), total[:-window]], axis=0
        )
        window *= 2
        picked = jnp.where(group == step, total[HALO:], picked)
    position = place_ref[0] + lax.broadcasted_iota(jnp.int32, rows.shape, 0)
    width = jnp.left_shift(2, group)
    counts = jnp.minimum(position + 1, width).astype(jnp.float32)
    out_ref[...] = (picked / counts - rows).astype(out_ref.dtype)


def pool(place, before, rows):
    return pl.pallas_call(
        pool_kernel,
        out_shape=jax.ShapeDtypeStruct(rows.shape, rows.dtype),
        in_specs=[SMEM, VMEM, VMEM],
        out_specs=VMEM,
        name="pool",
        compiler_params=room(8),
        cost_estimate=cost(1_000_000, 300_000),
    )(place, before, rows)


def side_by_side(blocks):
    return jnp.concatenate([blocks[i] for i in range(blocks.shape[0])], axis=1)


def finish(total, squares, width):
    units = total.shape[1] // 2
    inverse = lax.rsqrt(jnp.sum(squares, axis=1, keepdims=True) / width + norm_eps)
    gates, ups = total[:, :units] * inverse, total[:, units:] * inverse
    return (gates / (1.0 + jnp.exp(-gates)) * ups).astype(jnp.bfloat16)


def weights_kernel(gain_from, gate_from, up_from, out_ref, gain_ref, gate_ref, up_ref, sems):
    copies = [
        pltpu.make_async_copy(source, held, sems.at[i])
        for i, (source, held) in enumerate(
            ((gain_from, gain_ref), (gate_from, gate_ref), (up_from, up_ref))
        )
    ]
    for copy in copies:
        copy.start()
    for copy in copies:
        copy.wait()
    depth, units = gate_ref.shape[1:]
    for at in range(0, depth, 128):
        gain = jnp.broadcast_to(gain_ref[:, at : at + 128], (8, 128)).T[:, 0:1]
        for first, held in ((0, gate_ref), (units, up_ref)):
            out_ref[at : at + 128, first : first + units] = (
                held[0, at : at + 128].astype(jnp.float32) * gain
            ).astype(out_ref.dtype)


def scaled_weights(gain, gate_weight, up_weight):
    _, depth, units = gate_weight.shape
    return pl.pallas_call(
        weights_kernel,
        out_shape=jax.ShapeDtypeStruct((depth, 2 * units), jnp.bfloat16),
        in_specs=[HBM, HBM, HBM],
        out_specs=VMEM,
        scratch_shapes=[
            pltpu.VMEM(gain.shape, jnp.float32),
            pltpu.VMEM(gate_weight.shape, jnp.bfloat16),
            pltpu.VMEM(up_weight.shape, jnp.bfloat16),
            pltpu.SemaphoreType.DMA((3,)),
        ],
        name="weights",
        compiler_params=room(61),
        cost_estimate=cost(3_000_000, 4_200_000),
    )(gain, gate_weight, up_weight)


def products(rows, weight):
    square = 0.0
    for at in range(0, rows.shape[1], 128):
        square = square + jnp.square(rows[:, at : at + 128].astype(jnp.float32))
    return dot(rows, weight), square


def early_kernel(rows_ref, weight_ref, out_ref):
    total, square = products(side_by_side(rows_ref), weight_ref[...])
    out_ref[...] = finish(total, square, weight_ref.shape[0])


def early_hidden_of(gathered, weight):
    blocks, rows, features = gathered.shape
    units = weight.shape[1] // 2
    return pl.pallas_call(
        early_kernel,
        out_shape=jax.ShapeDtypeStruct((rows, units), jnp.bfloat16),
        in_specs=[VMEM] * 2,
        out_specs=VMEM,
        name="early_hidden",
        compiler_params=room(16),
        cost_estimate=cost(4 * rows * blocks * features * units, 3_500_000),
    )(gathered, weight)


def fetch(source_ref, first, held, sems):
    copies = []
    for block in range(held.shape[0]):
        piece = source_ref.at[block, pl.ds(first, held.shape[1])]
        copies.append(pltpu.make_async_copy(piece, held.at[block], sems.at[block]))
        copies[-1].start()
    return copies


def hidden_kernel(at_once, from_ref, weight_from, out_ref, held, weight_ref, sems, weight_sems):
    copies = fetch(from_ref, 0, held, sems)
    share = weight_ref.shape[0] // (len(copies) // at_once)
    weights = []
    for step in range(len(copies) // at_once):
        part = pl.ds(step * share, share)
        weights.append(
            pltpu.make_async_copy(weight_from.at[part], weight_ref.at[part], weight_sems.at[step])
        )
        weights[-1].start()
    rows = out_ref.shape[1]
    pieces = held.shape[1] // rows
    depth = at_once * pieces * held.shape[2]
    total = square = 0.0
    for step in range(len(copies) // at_once):
        parts = []
        for block in range(step * at_once, (step + 1) * at_once):
            copies[block].wait()
            parts += [held[block, i * rows : (i + 1) * rows] for i in range(pieces)]
        weights[step].wait()
        more, squares = products(
            jnp.concatenate(parts, axis=1), weight_ref[step * depth : (step + 1) * depth]
        )
        total, square = total + more, square + squares
    hidden = finish(total, square, weight_ref.shape[0])
    for copy in range(out_ref.shape[0]):
        out_ref[copy] = hidden


def hidden_of(gathered, weight, rows, pieces, copies):
    blocks, _, lanes = gathered.shape
    depth, both = weight.shape
    return pl.pallas_call(
        functools.partial(hidden_kernel, blocks // 2),
        out_shape=jax.ShapeDtypeStruct((copies, rows, both // 2), jnp.bfloat16),
        in_specs=[HBM, HBM],
        out_specs=VMEM,
        scratch_shapes=[
            pltpu.VMEM((blocks, pieces * rows, lanes), jnp.bfloat16),
            pltpu.VMEM(weight.shape, weight.dtype),
            pltpu.SemaphoreType.DMA((blocks,)),
            pltpu.SemaphoreType.DMA((2,)),
        ],
        name="hidden",
        compiler_params=pltpu.CompilerParams(vmem_limit_bytes=HOLD),
        cost_estimate=cost(2 * rows * depth * both, 6_500_000),
    )(gathered, weight)


def mix_kernel(at_once, first, from_ref, weight_ref, out_ref, held, sems):
    copies = fetch(from_ref, first, held, sems)
    depth = at_once * held.shape[2]
    total = 0.0
    for step in range(len(copies) // at_once):
        parts = []
        for block in range(step * at_once, (step + 1) * at_once):
            copies[block].wait()
            parts.append(held[block])
        part = weight_ref[step * depth : (step + 1) * depth]
        total = total + dot(jnp.concatenate(parts, axis=1), part)
    out_ref[...] = total.astype(out_ref.dtype)


def mixed_of(gathered, weight, first, rows):
    blocks, _, lanes = gathered.shape
    columns = weight.shape[1]
    return pl.pallas_call(
        functools.partial(mix_kernel, 4, first),
        out_shape=jax.ShapeDtypeStruct((rows, columns), jnp.bfloat16),
        in_specs=[HBM, VMEM],
        out_specs=VMEM,
        scratch_shapes=[
            pltpu.VMEM((blocks, rows, lanes), jnp.bfloat16),
            pltpu.SemaphoreType.DMA((blocks,)),
        ],
        name="mixed",
        compiler_params=room(60),
        cost_estimate=cost(2 * rows * blocks * lanes * columns, 3_500_000),
    )(gathered, weight)


def down_kernel(core_ref, early_ref, own_ref, other_ref, weight_ref, out_ref):
    core = core_ref[0]
    chips = own_ref.shape[0]
    units = early_ref.shape[2]
    split = early_ref.shape[1]
    weight = weight_ref[...].reshape(2 * chips * units, weight_ref.shape[2])
    out_ref[:split] = dot(side_by_side(early_ref), weight).astype(out_ref.dtype)
    mine = jnp.concatenate([weight_ref[2 * i + core] for i in range(chips)], axis=0)
    total = dot(side_by_side(own_ref), mine)
    theirs = jnp.concatenate([weight_ref[2 * i + 1 - core] for i in range(chips)], axis=0)
    out_ref[split:] = (total + dot(side_by_side(other_ref), theirs)).astype(out_ref.dtype)


def down(core, early, own, other, weight):
    columns = weight.shape[2]
    rows = early.shape[1] + own.shape[1]
    return pl.pallas_call(
        down_kernel,
        in_specs=[SMEM, VMEM, VMEM, VMEM, VMEM],
        out_specs=VMEM,
        out_shape=jax.ShapeDtypeStruct((rows, columns), jnp.bfloat16),
        name="down",
        compiler_params=room(16),
        cost_estimate=cost(2 * rows * weight.shape[0] * weight.shape[1] * columns, 3_500_000),
    )(core, early, own, other, weight)


def shards(
    mix_input,
    mix_weight,
    expert_input,
    expert_index,
    route_share,
    norm_gain,
    gate_weight,
    up_weight,
    down_weight,
):
    n_ep, n_tp = lax.axis_size("ep"), lax.axis_size("tp")
    chips = n_tp // 2
    ep, tp = lax.axis_index("ep"), lax.axis_index("tp")
    tokens_exp, features = expert_input.shape
    capacity = 2 * tokens_exp * TOP // n_ep
    units = gate_weight.shape[2]
    index, share, gain = expert_index.T, route_share.T, norm_gain.reshape(1, -1)

    weight = scaled_weights(gain, gate_weight, up_weight)

    outgoing = dispatch(index, expert_input, n_ep, capacity)
    outgoing = outgoing.reshape(n_ep, capacity, features)
    arrived = lax.all_to_all(outgoing, "ep", 0, 0, tiled=True).reshape(n_ep * capacity, features)

    tokens_mix, channels = mix_input.shape
    before = lax.ppermute(
        mix_input[tokens_mix - HALO :], "ep", [(i, i + 1) for i in range(n_ep - 1)]
    )
    place = jnp.stack([ep * tokens_mix, tp // (POOL // GROUPS // channels)]).astype(jnp.int32)
    pooled = pool(place, before, mix_input)

    arrived, weight = lax.optimization_barrier((arrived, weight))

    late_rows = n_ep * capacity - EARLY
    pieces = features // channels
    sent = [arrived[EARLY:, i * channels : (i + 1) * channels] for i in range(pieces)]
    gathered = lax.all_gather(jnp.concatenate(sent + [pooled], axis=0), "tp", axis=0)
    early = lax.all_gather(arrived[:EARLY], "tp", axis=0)
    early_hidden = early_hidden_of(early, weight)
    early_hidden = lax.all_gather(early_hidden, "tp", axis=0)
    gathered, early_hidden = lax.optimization_barrier((gathered, early_hidden))
    hidden = hidden_of(gathered, weight, late_rows, pieces, chips)
    mixed_rows = mixed_of(gathered, mix_weight, pieces * late_rows, tokens_mix)

    columns_of_chips = [[chip * 2 + core for chip in range(chips)] for core in range(2)]
    partners = [(i, i + 1 - 2 * (i % 2)) for i in range(n_tp)]
    own = lax.all_to_all(hidden, "tp", 0, 0, tiled=True, axis_index_groups=columns_of_chips)
    other = lax.ppermute(own, "tp", partners)
    core = lax.rem(tp, 2).astype(jnp.int32).reshape(1)
    produced = down(
        core, early_hidden, own, other, down_weight.reshape(n_tp, units, down_weight.shape[2])
    )

    returned = lax.all_to_all(
        produced.reshape(n_ep, capacity, produced.shape[1]), "ep", 0, 0, tiled=True
    )
    high, low = weights_of_slots(index, share, n_ep, capacity)
    expert_rows = combine(high, low, returned.reshape(n_ep * capacity, produced.shape[1]))
    return (mixed_rows, expert_rows)


def solution(mesh):
    placed = (
        P("ep", "tp"),
        P(None, "tp"),
        P("ep", "tp"),
        P("ep", None),
        P("ep", None),
        P(),
        P("ep", None, "tp"),
        P("ep", None, "tp"),
        P("ep", None, "tp"),
    )
    return jax.shard_map(
        shards,
        mesh=mesh,
        in_specs=placed,
        out_specs=(P("ep", "tp"), P("ep", "tp")),
        check_vma=False,
    )
```

```python
import functools

import jax
import jax.numpy as jnp
from jax import lax
from jax.experimental import pallas as pl
from jax.experimental.pallas import tpu as pltpu
from jax.sharding import PartitionSpec as P

POOL = 2048
GROUPS = 4
TOP = 2
HALO = 16
norm_eps = 1e-06

VMEM = pl.BlockSpec(memory_space=pltpu.VMEM)
SMEM = pl.BlockSpec(memory_space=pltpu.SMEM)
HBM = pl.BlockSpec(memory_space=pltpu.HBM)
HOLD = 588 * 2**20 // 10
EARLY = 112


def room(mib):
    return pltpu.CompilerParams(vmem_limit_bytes=mib * 2**20)


def cost(flops, moved):
    return pl.CostEstimate(flops=flops, bytes_accessed=moved, transcendentals=0)


def dot(a, b, dims=((1,), (0,))):
    return lax.dot_general(a, b, (dims, ((), ())), preferred_element_type=jnp.float32)


def slots_of(index, experts, capacity):
    tokens = index.shape[1]
    expert = lax.broadcasted_iota(jnp.int32, (experts, tokens), 0)
    first, second = expert == index[0:1], expert == index[1:2]
    named = jnp.where(first | second, 1.0, 0.0).astype(jnp.bfloat16)
    row = lax.broadcasted_iota(jnp.int32, (tokens, tokens), 0)
    col = lax.broadcasted_iota(jnp.int32, (tokens, tokens), 1)
    before = jnp.where(row < col, 1.0, 0.0).astype(jnp.bfloat16)
    slot = jnp.where(first | second, dot(named, before), -1.0).astype(jnp.bfloat16)
    place = lax.broadcasted_iota(jnp.int32, (experts * capacity, experts), 0)
    lane = lax.broadcasted_iota(jnp.int32, (experts * capacity, experts), 1)
    spread = jnp.where(place // capacity == lane, 1.0, 0.0).astype(jnp.bfloat16)
    wanted = lax.broadcasted_iota(jnp.int32, (experts * capacity, tokens), 0) % capacity
    hit = dot(spread, slot) == wanted.astype(jnp.float32)
    return hit, first, second, spread


def dispatch_kernel(experts, capacity, index_from, rows_from, out_ref, index_ref, rows_ref, sems):
    copies = [
        pltpu.make_async_copy(index_from, index_ref, sems.at[0]),
        pltpu.make_async_copy(rows_from, rows_ref, sems.at[1]),
    ]
    for copy in copies:
        copy.start()
    copies[0].wait()
    hit, _, _, _ = slots_of(index_ref[...], experts, capacity)
    placed = jnp.where(hit, 1.0, 0.0).astype(jnp.bfloat16)
    copies[1].wait()
    out_ref[...] = dot(placed, rows_ref[...]).astype(out_ref.dtype)


def dispatch(index, rows, experts, capacity):
    return pl.pallas_call(
        functools.partial(dispatch_kernel, experts, capacity),
        out_shape=jax.ShapeDtypeStruct((experts * capacity, rows.shape[1]), rows.dtype),
        in_specs=[HBM, HBM],
        out_specs=VMEM,
        scratch_shapes=[
            pltpu.VMEM(index.shape, index.dtype),
            pltpu.VMEM(rows.shape, rows.dtype),
            pltpu.SemaphoreType.DMA((2,)),
        ],
        name="dispatch",
        compiler_params=room(60),
        cost_estimate=cost(50_000_000, 400_000),
    )(index, rows)


def shares_kernel(experts, capacity, index_ref, share_ref, high_ref, low_ref):
    hit, first, second, spread = slots_of(index_ref[...], experts, capacity)
    share = share_ref[...]
    share = share / (share[0:1] + share[1:2])
    by_expert = jnp.where(first, share[0:1], jnp.where(second, share[1:2], 0.0))
    high = by_expert.astype(jnp.bfloat16)
    low = (by_expert - high.astype(jnp.float32)).astype(jnp.bfloat16)
    high_ref[...] = jnp.where(hit, dot(spread, high), 0.0).T.astype(jnp.bfloat16)
    low_ref[...] = jnp.where(hit, dot(spread, low), 0.0).T.astype(jnp.bfloat16)


def weights_of_slots(index, share, experts, capacity):
    shape = jax.ShapeDtypeStruct((index.shape[1], experts * capacity), jnp.bfloat16)
    return pl.pallas_call(
        functools.partial(shares_kernel, experts, capacity),
        out_shape=(shape, shape),
        in_specs=[VMEM, VMEM],
        out_specs=(VMEM, VMEM),
        name="shares",
        compiler_params=room(8),
        cost_estimate=cost(20_000_000, 300_000),
    )(index, share)


def combine_kernel(high_ref, low_ref, rows_ref, out_ref):
    rows = rows_ref[...]
    out_ref[...] = (dot(high_ref[...], rows) + dot(low_ref[...], rows)).astype(out_ref.dtype)


def combine(high, low, rows):
    return pl.pallas_call(
        combine_kernel,
        out_shape=jax.ShapeDtypeStruct((high.shape[0], rows.shape[1]), jnp.bfloat16),
        in_specs=[VMEM] * 3,
        out_specs=VMEM,
        name="combine",
        compiler_params=room(8),
        cost_estimate=cost(70_000_000, 600_000),
    )(high, low, rows)


def pool_kernel(place_ref, before_ref, rows_ref, out_ref):
    rows = rows_ref[...].astype(jnp.float32)
    total = jnp.concatenate([before_ref[...].astype(jnp.float32), rows], axis=0)
    group = place_ref[1]
    window = 1
    picked = jnp.zeros_like(rows)
    for step in range(GROUPS):
        total = total + jnp.concatenate(
            [jnp.zeros((window, total.shape[1]), jnp.float32), total[:-window]], axis=0
        )
        window *= 2
        picked = jnp.where(group == step, total[HALO:], picked)
    position = place_ref[0] + lax.broadcasted_iota(jnp.int32, rows.shape, 0)
    width = jnp.left_shift(2, group)
    counts = jnp.minimum(position + 1, width).astype(jnp.float32)
    out_ref[...] = (picked / counts - rows).astype(out_ref.dtype)


def pool(place, before, rows):
    return pl.pallas_call(
        pool_kernel,
        out_shape=jax.ShapeDtypeStruct(rows.shape, rows.dtype),
        in_specs=[SMEM, VMEM, VMEM],
        out_specs=VMEM,
        name="pool",
        compiler_params=room(8),
        cost_estimate=cost(1_000_000, 300_000),
    )(place, before, rows)


def side_by_side(blocks):
    return jnp.concatenate([blocks[i] for i in range(blocks.shape[0])], axis=1)


def finish(total, squares, width):
    units = total.shape[1] // 2
    inverse = lax.rsqrt(jnp.sum(squares, axis=1, keepdims=True) / width + norm_eps)
    gates, ups = total[:, :units] * inverse, total[:, units:] * inverse
    return (gates / (1.0 + jnp.exp(-gates)) * ups).astype(jnp.bfloat16)


def products(rows, gain, gate, up):
    rows = rows.astype(jnp.float32)
    scaled = (rows * gain).astype(jnp.bfloat16)
    square = jnp.square(rows)
    square = sum(square[:, at : at + 128] for at in range(0, rows.shape[1], 128))
    return dot(scaled, jnp.concatenate([gate, up], axis=1)), square


def early_kernel(rows_ref, gain_ref, gate_ref, up_ref, out_ref):
    total, square = products(side_by_side(rows_ref), gain_ref[...], gate_ref[0], up_ref[0])
    out_ref[...] = finish(total, square, gain_ref.shape[1])


def early_hidden_of(gathered, gain, gate_weight, up_weight):
    blocks, rows, features = gathered.shape
    units = gate_weight.shape[2]
    return pl.pallas_call(
        early_kernel,
        out_shape=jax.ShapeDtypeStruct((rows, units), jnp.bfloat16),
        in_specs=[VMEM] * 4,
        out_specs=VMEM,
        name="early_hidden",
        compiler_params=room(24),
        cost_estimate=cost(4 * rows * blocks * features * units, 3_500_000),
    )(gathered, gain, gate_weight, up_weight)


def fetch(source_ref, first, held, sems):
    copies = []
    for block in range(held.shape[0]):
        piece = source_ref.at[block, pl.ds(first, held.shape[1])]
        copies.append(pltpu.make_async_copy(piece, held.at[block], sems.at[block]))
        copies[-1].start()
    return copies


def hidden_kernel(
    at_once, from_ref, gain_ref, gate_from, up_from, out_ref, held, gate_ref, up_ref, sems, sides
):
    weights = [
        pltpu.make_async_copy(source, kept, sides.at[i])
        for i, (source, kept) in enumerate(((gate_from, gate_ref), (up_from, up_ref)))
    ]
    for weight in weights:
        weight.start()
    copies = fetch(from_ref, 0, held, sems)
    rows = out_ref.shape[1]
    pieces = held.shape[1] // rows
    depth = at_once * pieces * held.shape[2]
    total = square = 0.0
    for step in range(len(copies) // at_once):
        parts = []
        for block in range(step * at_once, (step + 1) * at_once):
            copies[block].wait()
            parts += [held[block, i * rows : (i + 1) * rows] for i in range(pieces)]
        if step == 0:
            for weight in weights:
                weight.wait()
        part = slice(step * depth, (step + 1) * depth)
        more, squares = products(
            jnp.concatenate(parts, axis=1), gain_ref[:, part], gate_ref[0, part], up_ref[0, part]
        )
        total, square = total + more, square + squares
    hidden = finish(total, square, gain_ref.shape[1])
    for copy in range(out_ref.shape[0]):
        out_ref[copy] = hidden


def hidden_of(gathered, gain, gate_weight, up_weight, rows, pieces, copies):
    blocks, _, lanes = gathered.shape
    units = gate_weight.shape[2]
    return pl.pallas_call(
        functools.partial(hidden_kernel, blocks // 2),
        out_shape=jax.ShapeDtypeStruct((copies, rows, units), jnp.bfloat16),
        in_specs=[HBM, VMEM, HBM, HBM],
        out_specs=VMEM,
        scratch_shapes=[
            pltpu.VMEM((blocks, pieces * rows, lanes), jnp.bfloat16),
            pltpu.VMEM(gate_weight.shape, jnp.bfloat16),
            pltpu.VMEM(up_weight.shape, jnp.bfloat16),
            pltpu.SemaphoreType.DMA((blocks,)),
            pltpu.SemaphoreType.DMA((2,)),
        ],
        name="hidden",
        compiler_params=pltpu.CompilerParams(vmem_limit_bytes=HOLD),
        cost_estimate=cost(4 * rows * gain.shape[1] * units, 6_500_000),
    )(gathered, gain, gate_weight, up_weight)


def mix_kernel(at_once, first, from_ref, weight_ref, out_ref, held, sems):
    copies = fetch(from_ref, first, held, sems)
    depth = at_once * held.shape[2]
    total = 0.0
    for step in range(len(copies) // at_once):
        parts = []
        for block in range(step * at_once, (step + 1) * at_once):
            copies[block].wait()
            parts.append(held[block])
        part = weight_ref[step * depth : (step + 1) * depth]
        total = total + dot(jnp.concatenate(parts, axis=1), part)
    out_ref[...] = total.astype(out_ref.dtype)


def mixed_of(gathered, weight, first, rows):
    blocks, _, lanes = gathered.shape
    columns = weight.shape[1]
    return pl.pallas_call(
        functools.partial(mix_kernel, 4, first),
        out_shape=jax.ShapeDtypeStruct((rows, columns), jnp.bfloat16),
        in_specs=[HBM, VMEM],
        out_specs=VMEM,
        scratch_shapes=[
            pltpu.VMEM((blocks, rows, lanes), jnp.bfloat16),
            pltpu.SemaphoreType.DMA((blocks,)),
        ],
        name="mixed",
        compiler_params=room(60),
        cost_estimate=cost(2 * rows * blocks * lanes * columns, 3_500_000),
    )(gathered, weight)


def down_kernel(core_ref, early_ref, own_ref, other_ref, weight_ref, out_ref):
    core = core_ref[0]
    chips = own_ref.shape[0]
    units = early_ref.shape[2]
    split = early_ref.shape[1]
    weight = weight_ref[...].reshape(2 * chips * units, weight_ref.shape[2])
    out_ref[:split] = dot(side_by_side(early_ref), weight).astype(out_ref.dtype)
    mine = jnp.concatenate([weight_ref[2 * i + core] for i in range(chips)], axis=0)
    total = dot(side_by_side(own_ref), mine)
    theirs = jnp.concatenate([weight_ref[2 * i + 1 - core] for i in range(chips)], axis=0)
    out_ref[split:] = (total + dot(side_by_side(other_ref), theirs)).astype(out_ref.dtype)


def down(core, early, own, other, weight):
    columns = weight.shape[2]
    rows = early.shape[1] + own.shape[1]
    return pl.pallas_call(
        down_kernel,
        in_specs=[SMEM, VMEM, VMEM, VMEM, VMEM],
        out_specs=VMEM,
        out_shape=jax.ShapeDtypeStruct((rows, columns), jnp.bfloat16),
        name="down",
        compiler_params=room(16),
        cost_estimate=cost(2 * rows * weight.shape[0] * weight.shape[1] * columns, 3_500_000),
    )(core, early, own, other, weight)


def shards(
    mix_input,
    mix_weight,
    expert_input,
    expert_index,
    route_share,
    norm_gain,
    gate_weight,
    up_weight,
    down_weight,
):
    n_ep, n_tp = lax.axis_size("ep"), lax.axis_size("tp")
    chips = n_tp // 2
    ep, tp = lax.axis_index("ep"), lax.axis_index("tp")
    tokens_exp, features = expert_input.shape
    capacity = 2 * tokens_exp * TOP // n_ep
    units = gate_weight.shape[2]
    index, share, gain = expert_index.T, route_share.T, norm_gain.reshape(1, -1)

    outgoing = dispatch(index, expert_input, n_ep, capacity)
    outgoing = outgoing.reshape(n_ep, capacity, features)
    arrived = lax.all_to_all(outgoing, "ep", 0, 0, tiled=True).reshape(n_ep * capacity, features)

    tokens_mix, channels = mix_input.shape
    before = lax.ppermute(
        mix_input[tokens_mix - HALO :], "ep", [(i, i + 1) for i in range(n_ep - 1)]
    )
    place = jnp.stack([ep * tokens_mix, tp // (POOL // GROUPS // channels)]).astype(jnp.int32)
    pooled = pool(place, before, mix_input)

    late_rows = n_ep * capacity - EARLY
    pieces = features // channels
    sent = [arrived[EARLY:, i * channels : (i + 1) * channels] for i in range(pieces)]
    gathered = lax.all_gather(jnp.concatenate(sent + [pooled], axis=0), "tp", axis=0)
    early = lax.all_gather(arrived[:EARLY], "tp", axis=0)
    early_hidden = early_hidden_of(early, gain, gate_weight, up_weight)
    early_hidden = lax.all_gather(early_hidden, "tp", axis=0)
    gathered, early_hidden = lax.optimization_barrier((gathered, early_hidden))
    hidden = hidden_of(gathered, gain, gate_weight, up_weight, late_rows, pieces, chips)
    mixed_rows = mixed_of(gathered, mix_weight, pieces * late_rows, tokens_mix)

    columns_of_chips = [[chip * 2 + core for chip in range(chips)] for core in range(2)]
    partners = [(i, i + 1 - 2 * (i % 2)) for i in range(n_tp)]
    own = lax.all_to_all(hidden, "tp", 0, 0, tiled=True, axis_index_groups=columns_of_chips)
    other = lax.ppermute(own, "tp", partners)
    core = lax.rem(tp, 2).astype(jnp.int32).reshape(1)
    produced = down(
        core, early_hidden, own, other, down_weight.reshape(n_tp, units, down_weight.shape[2])
    )

    returned = lax.all_to_all(
        produced.reshape(n_ep, capacity, produced.shape[1]), "ep", 0, 0, tiled=True
    )
    high, low = weights_of_slots(index, share, n_ep, capacity)
    expert_rows = combine(high, low, returned.reshape(n_ep * capacity, produced.shape[1]))
    return (mixed_rows, expert_rows)


def solution(mesh):
    placed = (
        P("ep", "tp"),
        P(None, "tp"),
        P("ep", "tp"),
        P("ep", None),
        P("ep", None),
        P(),
        P("ep", None, "tp"),
        P("ep", None, "tp"),
        P("ep", None, "tp"),
    )
    return jax.shard_map(
        shards,
        mesh=mesh,
        in_specs=placed,
        out_specs=(P("ep", "tp"), P("ep", "tp")),
        check_vma=False,
    )
```

```python
import functools

import jax
import jax.numpy as jnp
from jax import lax
from jax.experimental import pallas as pl
from jax.experimental.pallas import tpu as pltpu
from jax.sharding import PartitionSpec as P

POOL = 2048
GROUPS = 4
TOP = 2
HALO = 16
norm_eps = 1e-06

VMEM = pl.BlockSpec(memory_space=pltpu.VMEM)
SMEM = pl.BlockSpec(memory_space=pltpu.SMEM)
HBM = pl.BlockSpec(memory_space=pltpu.HBM)
EARLY = 112


def room(mib):
    return pltpu.CompilerParams(vmem_limit_bytes=mib * 2**20)


def cost(flops, moved):
    return pl.CostEstimate(flops=flops, bytes_accessed=moved, transcendentals=0)


def dot(a, b, dims=((1,), (0,))):
    return lax.dot_general(a, b, (dims, ((), ())), preferred_element_type=jnp.float32)


def slots_of(index, experts, capacity):
    tokens = index.shape[1]
    expert = lax.broadcasted_iota(jnp.int32, (experts, tokens), 0)
    first, second = expert == index[0:1], expert == index[1:2]
    named = jnp.where(first | second, 1.0, 0.0).astype(jnp.bfloat16)
    row = lax.broadcasted_iota(jnp.int32, (tokens, tokens), 0)
    col = lax.broadcasted_iota(jnp.int32, (tokens, tokens), 1)
    before = jnp.where(row < col, 1.0, 0.0).astype(jnp.bfloat16)
    slot = jnp.where(first | second, dot(named, before), -1.0).astype(jnp.bfloat16)
    place = lax.broadcasted_iota(jnp.int32, (experts * capacity, experts), 0)
    lane = lax.broadcasted_iota(jnp.int32, (experts * capacity, experts), 1)
    spread = jnp.where(place // capacity == lane, 1.0, 0.0).astype(jnp.bfloat16)
    wanted = lax.broadcasted_iota(jnp.int32, (experts * capacity, tokens), 0) % capacity
    hit = dot(spread, slot) == wanted.astype(jnp.float32)
    return hit, first, second, spread


def dispatch_kernel(experts, capacity, index_from, rows_from, out_ref, index_ref, rows_ref, sems):
    copies = [
        pltpu.make_async_copy(index_from, index_ref, sems.at[0]),
        pltpu.make_async_copy(rows_from, rows_ref, sems.at[1]),
    ]
    for copy in copies:
        copy.start()
    copies[0].wait()
    hit, _, _, _ = slots_of(index_ref[...], experts, capacity)
    placed = jnp.where(hit, 1.0, 0.0).astype(jnp.bfloat16)
    copies[1].wait()
    out_ref[...] = dot(placed, rows_ref[...]).astype(out_ref.dtype)


def dispatch(index, rows, experts, capacity):
    return pl.pallas_call(
        functools.partial(dispatch_kernel, experts, capacity),
        out_shape=jax.ShapeDtypeStruct((experts * capacity, rows.shape[1]), rows.dtype),
        in_specs=[HBM, HBM],
        out_specs=VMEM,
        scratch_shapes=[
            pltpu.VMEM(index.shape, index.dtype),
            pltpu.VMEM(rows.shape, rows.dtype),
            pltpu.SemaphoreType.DMA((2,)),
        ],
        name="dispatch",
        compiler_params=room(60),
        cost_estimate=cost(50_000_000, 400_000),
    )(index, rows)


def shares_kernel(experts, capacity, index_ref, share_ref, high_ref, low_ref):
    hit, first, second, spread = slots_of(index_ref[...], experts, capacity)
    share = share_ref[...]
    share = share / (share[0:1] + share[1:2])
    by_expert = jnp.where(first, share[0:1], jnp.where(second, share[1:2], 0.0))
    high = by_expert.astype(jnp.bfloat16)
    low = (by_expert - high.astype(jnp.float32)).astype(jnp.bfloat16)
    high_ref[...] = jnp.where(hit, dot(spread, high), 0.0).T.astype(jnp.bfloat16)
    low_ref[...] = jnp.where(hit, dot(spread, low), 0.0).T.astype(jnp.bfloat16)


def weights_of_slots(index, share, experts, capacity):
    shape = jax.ShapeDtypeStruct((index.shape[1], experts * capacity), jnp.bfloat16)
    return pl.pallas_call(
        functools.partial(shares_kernel, experts, capacity),
        out_shape=(shape, shape),
        in_specs=[VMEM, VMEM],
        out_specs=(VMEM, VMEM),
        name="shares",
        compiler_params=room(8),
        cost_estimate=cost(20_000_000, 300_000),
    )(index, share)


def combine_kernel(high_ref, low_ref, rows_ref, out_ref):
    rows = rows_ref[...]
    out_ref[...] = (dot(high_ref[...], rows) + dot(low_ref[...], rows)).astype(out_ref.dtype)


def combine(high, low, rows):
    return pl.pallas_call(
        combine_kernel,
        out_shape=jax.ShapeDtypeStruct((high.shape[0], rows.shape[1]), jnp.bfloat16),
        in_specs=[VMEM] * 3,
        out_specs=VMEM,
        name="combine",
        compiler_params=room(8),
        cost_estimate=cost(70_000_000, 600_000),
    )(high, low, rows)


def pool_kernel(place_ref, before_ref, rows_ref, out_ref):
    rows = rows_ref[...].astype(jnp.float32)
    total = jnp.concatenate([before_ref[...].astype(jnp.float32), rows], axis=0)
    group = place_ref[1]
    window = 1
    picked = jnp.zeros_like(rows)
    for step in range(GROUPS):
        total = total + jnp.concatenate(
            [jnp.zeros((window, total.shape[1]), jnp.float32), total[:-window]], axis=0
        )
        window *= 2
        picked = jnp.where(group == step, total[HALO:], picked)
    position = place_ref[0] + lax.broadcasted_iota(jnp.int32, rows.shape, 0)
    width = jnp.left_shift(2, group)
    counts = jnp.minimum(position + 1, width).astype(jnp.float32)
    out_ref[...] = (picked / counts - rows).astype(out_ref.dtype)


def pool(place, before, rows):
    return pl.pallas_call(
        pool_kernel,
        out_shape=jax.ShapeDtypeStruct(rows.shape, rows.dtype),
        in_specs=[SMEM, VMEM, VMEM],
        out_specs=VMEM,
        name="pool",
        compiler_params=room(8),
        cost_estimate=cost(1_000_000, 300_000),
    )(place, before, rows)


def side_by_side(blocks):
    return jnp.concatenate([blocks[i] for i in range(blocks.shape[0])], axis=1)


def finish(total, squares, width):
    units = total.shape[1] // 2
    inverse = lax.rsqrt(jnp.sum(squares, axis=1, keepdims=True) / width + norm_eps)
    gates, ups = total[:, :units] * inverse, total[:, units:] * inverse
    return (gates / (1.0 + jnp.exp(-gates)) * ups).astype(jnp.bfloat16)


def products(rows, gain, gate, up):
    rows = rows.astype(jnp.float32)
    scaled = (rows * gain).astype(jnp.bfloat16)
    square = jnp.square(rows)
    square = sum(square[:, at : at + 128] for at in range(0, rows.shape[1], 128))
    return dot(scaled, jnp.concatenate([gate, up], axis=1)), square


def early_kernel(rows_ref, gain_ref, gate_ref, up_ref, out_ref):
    total, square = products(side_by_side(rows_ref), gain_ref[...], gate_ref[0], up_ref[0])
    out_ref[...] = finish(total, square, gain_ref.shape[1])


def early_hidden_of(gathered, gain, gate_weight, up_weight):
    blocks, rows, features = gathered.shape
    units = gate_weight.shape[2]
    return pl.pallas_call(
        early_kernel,
        out_shape=jax.ShapeDtypeStruct((rows, units), jnp.bfloat16),
        in_specs=[VMEM] * 4,
        out_specs=VMEM,
        name="early_hidden",
        compiler_params=room(24),
        cost_estimate=cost(4 * rows * blocks * features * units, 3_500_000),
    )(gathered, gain, gate_weight, up_weight)


def fetch(source_ref, first, held, sems):
    copies = []
    for block in range(held.shape[0]):
        piece = source_ref.at[block, pl.ds(first, held.shape[1])]
        copies.append(pltpu.make_async_copy(piece, held.at[block], sems.at[block]))
        copies[-1].start()
    return copies


def hidden_kernel(
    at_once, from_ref, gain_ref, gate_ref, up_ref, out_ref, held, sems
):
    copies = fetch(from_ref, 0, held, sems)
    rows = out_ref.shape[1]
    pieces = held.shape[1] // rows
    depth = at_once * pieces * held.shape[2]
    total = square = 0.0
    for step in range(len(copies) // at_once):
        parts = []
        for block in range(step * at_once, (step + 1) * at_once):
            copies[block].wait()
            parts += [held[block, i * rows : (i + 1) * rows] for i in range(pieces)]
        part = slice(step * depth, (step + 1) * depth)
        more, squares = products(
            jnp.concatenate(parts, axis=1), gain_ref[:, part], gate_ref[0, part], up_ref[0, part]
        )
        total, square = total + more, square + squares
    hidden = finish(total, square, gain_ref.shape[1])
    for copy in range(out_ref.shape[0]):
        out_ref[copy] = hidden


def hidden_of(gathered, gain, gate_weight, up_weight, rows, pieces, copies):
    blocks, _, lanes = gathered.shape
    units = gate_weight.shape[2]
    return pl.pallas_call(
        functools.partial(hidden_kernel, blocks // 2),
        out_shape=jax.ShapeDtypeStruct((copies, rows, units), jnp.bfloat16),
        in_specs=[HBM, VMEM, VMEM, VMEM],
        out_specs=VMEM,
        scratch_shapes=[
            pltpu.VMEM((blocks, pieces * rows, lanes), jnp.bfloat16),
            pltpu.SemaphoreType.DMA((blocks,)),
        ],
        name="hidden",
        compiler_params=room(28),
        cost_estimate=cost(4 * rows * gain.shape[1] * units, 6_500_000),
    )(pltpu.with_memory_space_constraint(gathered, pltpu.HBM), gain, gate_weight, up_weight)


def mix_kernel(at_once, first, from_ref, weight_ref, out_ref, held, sems):
    copies = fetch(from_ref, first, held, sems)
    depth = at_once * held.shape[2]
    total = 0.0
    for step in range(len(copies) // at_once):
        parts = []
        for block in range(step * at_once, (step + 1) * at_once):
            copies[block].wait()
            parts.append(held[block])
        part = weight_ref[step * depth : (step + 1) * depth]
        total = total + dot(jnp.concatenate(parts, axis=1), part)
    out_ref[...] = total.astype(out_ref.dtype)


def mixed_of(gathered, weight, first, rows):
    blocks, _, lanes = gathered.shape
    columns = weight.shape[1]
    return pl.pallas_call(
        functools.partial(mix_kernel, 4, first),
        out_shape=jax.ShapeDtypeStruct((rows, columns), jnp.bfloat16),
        in_specs=[HBM, VMEM],
        out_specs=VMEM,
        scratch_shapes=[
            pltpu.VMEM((blocks, rows, lanes), jnp.bfloat16),
            pltpu.SemaphoreType.DMA((blocks,)),
        ],
        name="mixed",
        compiler_params=room(24),
        cost_estimate=cost(2 * rows * blocks * lanes * columns, 3_500_000),
    )(pltpu.with_memory_space_constraint(gathered, pltpu.HBM), weight)


def down_kernel(core_ref, early_ref, own_ref, other_ref, weight_ref, out_ref):
    core = core_ref[0]
    chips = own_ref.shape[0]
    units = early_ref.shape[2]
    split = early_ref.shape[1]
    weight = weight_ref[...].reshape(2 * chips * units, weight_ref.shape[2])
    out_ref[:split] = dot(side_by_side(early_ref), weight).astype(out_ref.dtype)
    mine = jnp.concatenate([weight_ref[2 * i + core] for i in range(chips)], axis=0)
    total = dot(side_by_side(own_ref), mine)
    theirs = jnp.concatenate([weight_ref[2 * i + 1 - core] for i in range(chips)], axis=0)
    out_ref[split:] = (total + dot(side_by_side(other_ref), theirs)).astype(out_ref.dtype)


def down(core, early, own, other, weight):
    columns = weight.shape[2]
    rows = early.shape[1] + own.shape[1]
    return pl.pallas_call(
        down_kernel,
        in_specs=[SMEM, VMEM, VMEM, VMEM, VMEM],
        out_specs=VMEM,
        out_shape=jax.ShapeDtypeStruct((rows, columns), jnp.bfloat16),
        name="down",
        compiler_params=room(16),
        cost_estimate=cost(2 * rows * weight.shape[0] * weight.shape[1] * columns, 3_500_000),
    )(core, early, own, other, weight)


def shards(
    mix_input,
    mix_weight,
    expert_input,
    expert_index,
    route_share,
    norm_gain,
    gate_weight,
    up_weight,
    down_weight,
):
    n_ep, n_tp = lax.axis_size("ep"), lax.axis_size("tp")
    chips = n_tp // 2
    ep, tp = lax.axis_index("ep"), lax.axis_index("tp")
    tokens_exp, features = expert_input.shape
    capacity = 2 * tokens_exp * TOP // n_ep
    units = gate_weight.shape[2]
    index, share, gain = expert_index.T, route_share.T, norm_gain.reshape(1, -1)

    outgoing = dispatch(index, expert_input, n_ep, capacity)
    outgoing = outgoing.reshape(n_ep, capacity, features)
    arrived = lax.all_to_all(outgoing, "ep", 0, 0, tiled=True).reshape(n_ep * capacity, features)

    tokens_mix, channels = mix_input.shape
    before = lax.ppermute(
        mix_input[tokens_mix - HALO :], "ep", [(i, i + 1) for i in range(n_ep - 1)]
    )
    place = jnp.stack([ep * tokens_mix, tp // (POOL // GROUPS // channels)]).astype(jnp.int32)
    pooled = pool(place, before, mix_input)

    late_rows = n_ep * capacity - EARLY
    pieces = features // channels
    sent = [arrived[EARLY:, i * channels : (i + 1) * channels] for i in range(pieces)]
    gathered = lax.all_gather(jnp.concatenate(sent + [pooled], axis=0), "tp", axis=0)
    early = lax.all_gather(arrived[:EARLY], "tp", axis=0)
    early_hidden = early_hidden_of(early, gain, gate_weight, up_weight)
    early_hidden = lax.all_gather(early_hidden, "tp", axis=0)
    gathered, early_hidden = lax.optimization_barrier((gathered, early_hidden))
    hidden = hidden_of(gathered, gain, gate_weight, up_weight, late_rows, pieces, chips)
    mixed_rows = mixed_of(gathered, mix_weight, pieces * late_rows, tokens_mix)

    columns_of_chips = [[chip * 2 + core for chip in range(chips)] for core in range(2)]
    partners = [(i, i + 1 - 2 * (i % 2)) for i in range(n_tp)]
    own = lax.all_to_all(hidden, "tp", 0, 0, tiled=True, axis_index_groups=columns_of_chips)
    other = lax.ppermute(own, "tp", partners)
    core = lax.rem(tp, 2).astype(jnp.int32).reshape(1)
    produced = down(
        core, early_hidden, own, other, down_weight.reshape(n_tp, units, down_weight.shape[2])
    )

    returned = lax.all_to_all(
        produced.reshape(n_ep, capacity, produced.shape[1]), "ep", 0, 0, tiled=True
    )
    high, low = weights_of_slots(index, share, n_ep, capacity)
    expert_rows = combine(high, low, returned.reshape(n_ep * capacity, produced.shape[1]))
    return (mixed_rows, expert_rows)


def solution(mesh):
    placed = (
        P("ep", "tp"),
        P(None, "tp"),
        P("ep", "tp"),
        P("ep", None),
        P("ep", None),
        P(),
        P("ep", None, "tp"),
        P("ep", None, "tp"),
        P("ep", None, "tp"),
    )
    return jax.shard_map(
        shards,
        mesh=mesh,
        in_specs=placed,
        out_specs=(P("ep", "tp"), P("ep", "tp")),
        check_vma=False,
    )
```

```python
import functools

import jax
import jax.numpy as jnp
from jax import lax
from jax.experimental import pallas as pl
from jax.experimental.pallas import tpu as pltpu
from jax.sharding import PartitionSpec as P

POOL = 2048
GROUPS = 4
TOP = 2
HALO = 16
norm_eps = 1e-06

VMEM = pl.BlockSpec(memory_space=pltpu.VMEM)
SMEM = pl.BlockSpec(memory_space=pltpu.SMEM)
HBM = pl.BlockSpec(memory_space=pltpu.HBM)
EARLY = 120


def room(mib):
    return pltpu.CompilerParams(vmem_limit_bytes=mib * 2**20)


def cost(flops, moved):
    return pl.CostEstimate(flops=flops, bytes_accessed=moved, transcendentals=0)


def dot(a, b, dims=((1,), (0,))):
    return lax.dot_general(a, b, (dims, ((), ())), preferred_element_type=jnp.float32)


def slots_of(index, experts, capacity):
    tokens = index.shape[1]
    expert = lax.broadcasted_iota(jnp.int32, (experts, tokens), 0)
    first, second = expert == index[0:1], expert == index[1:2]
    named = jnp.where(first | second, 1.0, 0.0).astype(jnp.bfloat16)
    row = lax.broadcasted_iota(jnp.int32, (tokens, tokens), 0)
    col = lax.broadcasted_iota(jnp.int32, (tokens, tokens), 1)
    before = jnp.where(row < col, 1.0, 0.0).astype(jnp.bfloat16)
    slot = jnp.where(first | second, dot(named, before), -1.0).astype(jnp.bfloat16)
    place = lax.broadcasted_iota(jnp.int32, (experts * capacity, experts), 0)
    lane = lax.broadcasted_iota(jnp.int32, (experts * capacity, experts), 1)
    spread = jnp.where(place // capacity == lane, 1.0, 0.0).astype(jnp.bfloat16)
    wanted = lax.broadcasted_iota(jnp.int32, (experts * capacity, tokens), 0) % capacity
    hit = dot(spread, slot) == wanted.astype(jnp.float32)
    return hit, first, second, spread


def dispatch_kernel(experts, capacity, index_from, rows_from, out_ref, index_ref, rows_ref, sems):
    copies = [
        pltpu.make_async_copy(index_from, index_ref, sems.at[0]),
        pltpu.make_async_copy(rows_from, rows_ref, sems.at[1]),
    ]
    for copy in copies:
        copy.start()
    copies[0].wait()
    hit, _, _, _ = slots_of(index_ref[...], experts, capacity)
    placed = jnp.where(hit, 1.0, 0.0).astype(jnp.bfloat16)
    copies[1].wait()
    out_ref[...] = dot(placed, rows_ref[...]).astype(out_ref.dtype)


def dispatch(index, rows, experts, capacity):
    return pl.pallas_call(
        functools.partial(dispatch_kernel, experts, capacity),
        out_shape=jax.ShapeDtypeStruct((experts * capacity, rows.shape[1]), rows.dtype),
        in_specs=[HBM, HBM],
        out_specs=VMEM,
        scratch_shapes=[
            pltpu.VMEM(index.shape, index.dtype),
            pltpu.VMEM(rows.shape, rows.dtype),
            pltpu.SemaphoreType.DMA((2,)),
        ],
        name="dispatch",
        compiler_params=room(60),
        cost_estimate=cost(50_000_000, 400_000),
    )(index, rows)


def shares_kernel(experts, capacity, index_ref, share_ref, high_ref, low_ref):
    hit, first, second, spread = slots_of(index_ref[...], experts, capacity)
    share = share_ref[...]
    share = share / (share[0:1] + share[1:2])
    by_expert = jnp.where(first, share[0:1], jnp.where(second, share[1:2], 0.0))
    high = by_expert.astype(jnp.bfloat16)
    low = (by_expert - high.astype(jnp.float32)).astype(jnp.bfloat16)
    high_ref[...] = jnp.where(hit, dot(spread, high), 0.0).T.astype(jnp.bfloat16)
    low_ref[...] = jnp.where(hit, dot(spread, low), 0.0).T.astype(jnp.bfloat16)


def weights_of_slots(index, share, experts, capacity):
    shape = jax.ShapeDtypeStruct((index.shape[1], experts * capacity), jnp.bfloat16)
    return pl.pallas_call(
        functools.partial(shares_kernel, experts, capacity),
        out_shape=(shape, shape),
        in_specs=[VMEM, VMEM],
        out_specs=(VMEM, VMEM),
        name="shares",
        compiler_params=room(8),
        cost_estimate=cost(20_000_000, 300_000),
    )(index, share)


def combine_kernel(high_ref, low_ref, rows_ref, out_ref):
    rows = rows_ref[...]
    out_ref[...] = (dot(high_ref[...], rows) + dot(low_ref[...], rows)).astype(out_ref.dtype)


def combine(high, low, rows):
    return pl.pallas_call(
        combine_kernel,
        out_shape=jax.ShapeDtypeStruct((high.shape[0], rows.shape[1]), jnp.bfloat16),
        in_specs=[VMEM] * 3,
        out_specs=VMEM,
        name="combine",
        compiler_params=room(8),
        cost_estimate=cost(70_000_000, 600_000),
    )(high, low, rows)


def pool_kernel(place_ref, before_ref, rows_ref, out_ref):
    rows = rows_ref[...].astype(jnp.float32)
    total = jnp.concatenate([before_ref[...].astype(jnp.float32), rows], axis=0)
    group = place_ref[1]
    window = 1
    picked = jnp.zeros_like(rows)
    for step in range(GROUPS):
        total = total + jnp.concatenate(
            [jnp.zeros((window, total.shape[1]), jnp.float32), total[:-window]], axis=0
        )
        window *= 2
        picked = jnp.where(group == step, total[HALO:], picked)
    position = place_ref[0] + lax.broadcasted_iota(jnp.int32, rows.shape, 0)
    width = jnp.left_shift(2, group)
    counts = jnp.minimum(position + 1, width).astype(jnp.float32)
    out_ref[...] = (picked / counts - rows).astype(out_ref.dtype)


def pool(place, before, rows):
    return pl.pallas_call(
        pool_kernel,
        out_shape=jax.ShapeDtypeStruct(rows.shape, rows.dtype),
        in_specs=[SMEM, VMEM, VMEM],
        out_specs=VMEM,
        name="pool",
        compiler_params=room(8),
        cost_estimate=cost(1_000_000, 300_000),
    )(place, before, rows)


def side_by_side(blocks):
    return jnp.concatenate([blocks[i] for i in range(blocks.shape[0])], axis=1)


def finish(total, squares, width):
    units = total.shape[1] // 2
    inverse = lax.rsqrt(jnp.sum(squares, axis=1, keepdims=True) / width + norm_eps)
    gates, ups = total[:, :units] * inverse, total[:, units:] * inverse
    return (gates / (1.0 + jnp.exp(-gates)) * ups).astype(jnp.bfloat16)


def products(rows, gain, gate, up):
    rows = rows.astype(jnp.float32)
    scaled = (rows * gain).astype(jnp.bfloat16)
    square = jnp.square(rows)
    square = sum(square[:, at : at + 128] for at in range(0, rows.shape[1], 128))
    return dot(scaled, jnp.concatenate([gate, up], axis=1)), square


def early_kernel(rows_ref, gain_ref, gate_ref, up_ref, out_ref):
    total, square = products(side_by_side(rows_ref), gain_ref[...], gate_ref[0], up_ref[0])
    out_ref[...] = finish(total, square, gain_ref.shape[1])


def early_hidden_of(gathered, gain, gate_weight, up_weight):
    blocks, rows, features = gathered.shape
    units = gate_weight.shape[2]
    return pl.pallas_call(
        early_kernel,
        out_shape=jax.ShapeDtypeStruct((rows, units), jnp.bfloat16),
        in_specs=[VMEM] * 4,
        out_specs=VMEM,
        name="early_hidden",
        compiler_params=room(24),
        cost_estimate=cost(4 * rows * blocks * features * units, 3_500_000),
    )(gathered, gain, gate_weight, up_weight)


def fetch(source_ref, first, held, sems):
    copies = []
    for block in range(held.shape[0]):
        piece = source_ref.at[block, pl.ds(first, held.shape[1])]
        copies.append(pltpu.make_async_copy(piece, held.at[block], sems.at[block]))
        copies[-1].start()
    return copies


def hidden_kernel(
    at_once, from_ref, gain_ref, gate_ref, up_ref, out_ref, held, sems
):
    copies = fetch(from_ref, 0, held, sems)
    rows = out_ref.shape[1]
    pieces = held.shape[1] // rows
    depth = at_once * pieces * held.shape[2]
    total = square = 0.0
    for step in range(len(copies) // at_once):
        parts = []
        for block in range(step * at_once, (step + 1) * at_once):
            copies[block].wait()
            parts += [held[block, i * rows : (i + 1) * rows] for i in range(pieces)]
        part = slice(step * depth, (step + 1) * depth)
        more, squares = products(
            jnp.concatenate(parts, axis=1), gain_ref[:, part], gate_ref[0, part], up_ref[0, part]
        )
        total, square = total + more, square + squares
    hidden = finish(total, square, gain_ref.shape[1])
    for copy in range(out_ref.shape[0]):
        out_ref[copy] = hidden


def hidden_of(gathered, gain, gate_weight, up_weight, rows, pieces, copies):
    blocks, _, lanes = gathered.shape
    units = gate_weight.shape[2]
    return pl.pallas_call(
        functools.partial(hidden_kernel, blocks // 2),
        out_shape=jax.ShapeDtypeStruct((copies, rows, units), jnp.bfloat16),
        in_specs=[HBM, VMEM, VMEM, VMEM],
        out_specs=VMEM,
        scratch_shapes=[
            pltpu.VMEM((blocks, pieces * rows, lanes), jnp.bfloat16),
            pltpu.SemaphoreType.DMA((blocks,)),
        ],
        name="hidden",
        compiler_params=room(28),
        cost_estimate=cost(4 * rows * gain.shape[1] * units, 6_500_000),
    )(pltpu.with_memory_space_constraint(gathered, pltpu.HBM), gain, gate_weight, up_weight)


def mix_kernel(at_once, first, from_ref, weight_ref, out_ref, held, sems):
    copies = fetch(from_ref, first, held, sems)
    depth = at_once * held.shape[2]
    total = 0.0
    for step in range(len(copies) // at_once):
        parts = []
        for block in range(step * at_once, (step + 1) * at_once):
            copies[block].wait()
            parts.append(held[block])
        part = weight_ref[step * depth : (step + 1) * depth]
        total = total + dot(jnp.concatenate(parts, axis=1), part)
    out_ref[...] = total.astype(out_ref.dtype)


def mixed_of(gathered, weight, first, rows):
    blocks, _, lanes = gathered.shape
    columns = weight.shape[1]
    return pl.pallas_call(
        functools.partial(mix_kernel, 4, first),
        out_shape=jax.ShapeDtypeStruct((rows, columns), jnp.bfloat16),
        in_specs=[HBM, VMEM],
        out_specs=VMEM,
        scratch_shapes=[
            pltpu.VMEM((blocks, rows, lanes), jnp.bfloat16),
            pltpu.SemaphoreType.DMA((blocks,)),
        ],
        name="mixed",
        compiler_params=room(24),
        cost_estimate=cost(2 * rows * blocks * lanes * columns, 3_500_000),
    )(pltpu.with_memory_space_constraint(gathered, pltpu.HBM), weight)


def down_kernel(core_ref, early_ref, own_ref, other_ref, weight_ref, out_ref):
    core = core_ref[0]
    chips = own_ref.shape[0]
    units = early_ref.shape[2]
    split = early_ref.shape[1]
    weight = weight_ref[...].reshape(2 * chips * units, weight_ref.shape[2])
    out_ref[:split] = dot(side_by_side(early_ref), weight).astype(out_ref.dtype)
    mine = jnp.concatenate([weight_ref[2 * i + core] for i in range(chips)], axis=0)
    total = dot(side_by_side(own_ref), mine)
    theirs = jnp.concatenate([weight_ref[2 * i + 1 - core] for i in range(chips)], axis=0)
    out_ref[split:] = (total + dot(side_by_side(other_ref), theirs)).astype(out_ref.dtype)


def down(core, early, own, other, weight):
    columns = weight.shape[2]
    rows = early.shape[1] + own.shape[1]
    return pl.pallas_call(
        down_kernel,
        in_specs=[SMEM, VMEM, VMEM, VMEM, VMEM],
        out_specs=VMEM,
        out_shape=jax.ShapeDtypeStruct((rows, columns), jnp.bfloat16),
        name="down",
        compiler_params=room(16),
        cost_estimate=cost(2 * rows * weight.shape[0] * weight.shape[1] * columns, 3_500_000),
    )(core, early, own, other, weight)


def shards(
    mix_input,
    mix_weight,
    expert_input,
    expert_index,
    route_share,
    norm_gain,
    gate_weight,
    up_weight,
    down_weight,
):
    n_ep, n_tp = lax.axis_size("ep"), lax.axis_size("tp")
    chips = n_tp // 2
    ep, tp = lax.axis_index("ep"), lax.axis_index("tp")
    tokens_exp, features = expert_input.shape
    capacity = 2 * tokens_exp * TOP // n_ep
    units = gate_weight.shape[2]
    index, share, gain = expert_index.T, route_share.T, norm_gain.reshape(1, -1)

    outgoing = dispatch(index, expert_input, n_ep, capacity)
    outgoing = outgoing.reshape(n_ep, capacity, features)
    arrived = lax.all_to_all(outgoing, "ep", 0, 0, tiled=True).reshape(n_ep * capacity, features)

    tokens_mix, channels = mix_input.shape
    before = lax.ppermute(
        mix_input[tokens_mix - HALO :], "ep", [(i, i + 1) for i in range(n_ep - 1)]
    )
    place = jnp.stack([ep * tokens_mix, tp // (POOL // GROUPS // channels)]).astype(jnp.int32)
    pooled = pool(place, before, mix_input)

    late_rows = n_ep * capacity - EARLY
    pieces = features // channels
    sent = [arrived[EARLY:, i * channels : (i + 1) * channels] for i in range(pieces)]
    gathered = lax.all_gather(jnp.concatenate(sent + [pooled], axis=0), "tp", axis=0)
    early = lax.all_gather(arrived[:EARLY], "tp", axis=0)
    early_hidden = early_hidden_of(early, gain, gate_weight, up_weight)
    early_hidden = lax.all_gather(early_hidden, "tp", axis=0)
    gathered, early_hidden = lax.optimization_barrier((gathered, early_hidden))
    hidden = hidden_of(gathered, gain, gate_weight, up_weight, late_rows, pieces, chips)
    mixed_rows = mixed_of(gathered, mix_weight, pieces * late_rows, tokens_mix)

    columns_of_chips = [[chip * 2 + core for chip in range(chips)] for core in range(2)]
    partners = [(i, i + 1 - 2 * (i % 2)) for i in range(n_tp)]
    own = lax.all_to_all(hidden, "tp", 0, 0, tiled=True, axis_index_groups=columns_of_chips)
    other = lax.ppermute(own, "tp", partners)
    core = lax.rem(tp, 2).astype(jnp.int32).reshape(1)
    produced = down(
        core, early_hidden, own, other, down_weight.reshape(n_tp, units, down_weight.shape[2])
    )

    returned = lax.all_to_all(
        produced.reshape(n_ep, capacity, produced.shape[1]), "ep", 0, 0, tiled=True
    )
    high, low = weights_of_slots(index, share, n_ep, capacity)
    expert_rows = combine(high, low, returned.reshape(n_ep * capacity, produced.shape[1]))
    return (mixed_rows, expert_rows)


def solution(mesh):
    placed = (
        P("ep", "tp"),
        P(None, "tp"),
        P("ep", "tp"),
        P("ep", None),
        P("ep", None),
        P(),
        P("ep", None, "tp"),
        P("ep", None, "tp"),
        P("ep", None, "tp"),
    )
    return jax.shard_map(
        shards,
        mesh=mesh,
        in_specs=placed,
        out_specs=(P("ep", "tp"), P("ep", "tp")),
        check_vma=False,
    )
```
